32 devices in a mesh: ep: 4 (over y, x), tp: 8 (over z, core).
Axes of the slice: x: 2, y: 2, z: 4, core: 2. Of those that a mesh axis runs over, the one named last changes fastest.
Arguments:
- queries: bfloat16 [4096, 1024], P('ep', 'tp'), may hold values from -12 to 12
- keys: bfloat16 [4096, 1024], P('ep', 'tp'), may hold values from -12 to 12
- values: bfloat16 [4096, 2048], P('ep', 'tp'), may hold values from -6 to 6
- out_gate: bfloat16 [4096, 2048], P('ep', 'tp'), may hold values from -6 to 6
- in_gate: float32 [16, 4096], P('tp', 'ep'), may hold values from -8 to 100
- forget_gate: float32 [16, 4096], P('tp', 'ep'), may hold values from 0 to 16
- out_gain: float32 [2048], P('tp'), may hold values from 0.1 to 1.9
- out_weight: bfloat16 [2048, 4096], P('tp'), may hold values from -0.1875 to 0.1875
- moe_rows: bfloat16 [512, 4096], P('ep'), may hold values from -36 to 36
- moe_gain: float32 [4096], replicated, may hold values from 0.1 to 1.9
- routes: int32 [512, 2], P('ep'), may hold values from 0 to 3, all different within a row; in each aligned block of 128 rows (0 to 127, 128 to 255, ...) at most 96 rows name the same one
- route_weight: float32 [512, 2], P('ep'), may hold values from 0.2 to 1.2
- expert_gate: bfloat16 [4, 4096, 4096], P('ep', None, 'tp'), may hold values from -0.09375 to 0.09375
- expert_up: bfloat16 [4, 4096, 4096], P('ep', None, 'tp'), may hold values from -0.09375 to 0.09375
- expert_down: bfloat16 [4, 4096, 4096], P('ep', 'tp'), may hold values from -0.125 to 0.125
- shared_gate: bfloat16 [4096, 2048], P(None, 'tp'), may hold values from -0.09375 to 0.09375
- shared_up: bfloat16 [4096, 2048], P(None, 'tp'), may hold values from -0.09375 to 0.09375
- shared_down: bfloat16 [2048, 4096], P('tp'), may hold values from -0.1875 to 0.1875
Outputs:
- mixer_out: bfloat16 [4096, 4096], P('ep', 'tp')
- moe_out: bfloat16 [512, 4096], P('ep', 'tp')
The draws below stay inside these ranges and needn't reach their ends.
Inputs may be any that keep to these rules, and one draw needn't show every extreme that they name: `routes`: each row names 2 different experts. Within the 128 rows of one index of ep no expert is named more than 96 times, a bound that some block reaches.
All inputs are finite; a program needn't handle non-finite values.
Results may differ from the reference program's by a relative error of at most 0.019.
Values may be sent and summed in bfloat16 or wider, within the bound.
No kernel may reach another device: no remote copies, remote signals or barrier semaphores. Data moves between devices by JAX's collectives and lax.ppermute only.
A program may use at most 128 MiB of HBM per device.

```python
import math
import jax
import jax.numpy as jnp
import numpy as np
from jax import lax

D = 4096
CELL_HEADS = 16
DK = 64
DV = 128
BLK = 64
TA_DEV = 1024
FE = 4096
FS = 2048
TOPK = 2
TB_DEV = 128
HW = 2048
SEQUENCE_TOKENS = 4096
TOKB = 512
EXPERTS = 4
CAP = 96
N_EP = 4
N_TP = 8


def draw_forget_gate(key, part):
    split_random_keys = jax.random.split(jax.random.fold_in(key, 11), 7)
    slow_share = 0.5
    slow_head = jax.random.bernoulli(split_random_keys[0], slow_share, (CELL_HEADS, 1))
    token_position = jnp.arange(SEQUENCE_TOKENS)
    slow_total = jnp.exp(jax.random.uniform(split_random_keys[1], (CELL_HEADS, 1), minval=jnp.log(0.15), maxval=jnp.log(0.5)))
    slow_rate = slow_total / SEQUENCE_TOKENS
    fast_rate = 1.0 / jnp.exp(jax.random.uniform(split_random_keys[2], (CELL_HEADS, 1), minval=jnp.log(20.0), maxval=jnp.log(60.0)))
    forget_decay_speed = jnp.where(slow_head, slow_rate, fast_rate)
    owner = token_position // TA_DEV
    jitter = jnp.exp(jax.random.uniform(split_random_keys[3], (CELL_HEADS, SEQUENCE_TOKENS // TA_DEV), minval=-0.2, maxval=0.2))
    device_factor = (2.0 ** (owner % 2).astype(jnp.float32))[None, :] * jnp.take(jitter, owner, axis=1)
    noise = jnp.exp(jax.random.uniform(split_random_keys[4], (CELL_HEADS, SEQUENCE_TOKENS), minval=-0.5, maxval=0.5))
    forget_decay_speed = forget_decay_speed * device_factor * noise
    spike_location = jax.random.randint(split_random_keys[5], (CELL_HEADS, 2, 1), 0, SEQUENCE_TOKENS)
    spike_reached = jnp.any(token_position[None, None, :] == spike_location, axis=1)
    spike_penalty = jax.random.uniform(split_random_keys[6], (CELL_HEADS, SEQUENCE_TOKENS), minval=0.2, maxval=0.45)
    forget_decay_speed = jnp.where(spike_reached, -jnp.log(1.0 - spike_penalty), forget_decay_speed)
    return (-jnp.log(jnp.expm1(forget_decay_speed))).astype(jnp.float32)


def draw_in_gate(key, part):
    split_random_keys = jax.random.split(jax.random.fold_in(key, 23), 2)
    return jnp.clip(1.5 * jax.random.normal(split_random_keys[1], (CELL_HEADS, SEQUENCE_TOKENS)), -8.0, 8.0).astype(jnp.float32)


def draw_moe_rows(key, part):
    split_random_keys = jax.random.split(jax.random.fold_in(key, 37), 3)
    row_scale = jnp.exp(jax.random.uniform(split_random_keys[0], (TOKB, 1), minval=jnp.log(0.3), maxval=jnp.log(3.0)))
    col_scale = jnp.exp(jax.random.uniform(split_random_keys[1], (1, D), minval=jnp.log(0.5), maxval=jnp.log(2.0)))
    base_draw = jax.random.normal(split_random_keys[2], (TOKB, D))
    return (jnp.clip(base_draw, -6.0, 6.0) * row_scale * col_scale).astype(jnp.bfloat16)


def common_direction(key):
    base = jax.random.normal(jax.random.fold_in(key, 51), (CELL_HEADS, DK))
    unit = base / jnp.sqrt(jnp.sum(base * base, axis=1, keepdims=True))
    return (8.0 * unit).reshape(1, CELL_HEADS * DK)


def draw_queries(key, part):
    noise_key = jax.random.fold_in(key, 61)
    noise = jnp.clip(jax.random.normal(noise_key, (SEQUENCE_TOKENS, CELL_HEADS * DK)), -4.0, 4.0)
    return (noise + common_direction(key)).astype(jnp.bfloat16)


def draw_keys(key, part):
    noise_key = jax.random.fold_in(key, 71)
    noise = jnp.clip(jax.random.normal(noise_key, (SEQUENCE_TOKENS, CELL_HEADS * DK)), -4.0, 4.0)
    return (noise + common_direction(key)).astype(jnp.bfloat16)


def strengthened(drawn, key, source, target, shards_of, factor):
    owner, partner = [(jnp.arange(drawn.shape[axis_at]) // (drawn.shape[axis_at] // shards_of)).reshape([-1 if axis == axis_at else 1 for axis in range(drawn.ndim)]) for axis_at in (source, target)]
    chosen = jax.random.permutation(key, shards_of)[partner]
    strong = (owner == chosen) | (owner == (partner + shards_of // 2) % shards_of)
    return jnp.where(strong, factor * drawn, drawn)


def block_levels(rng, dims, shards, low, high):
    def one(axis_at, parts):
        heights = jax.random.uniform(jax.random.fold_in(jax.random.fold_in(rng, 6), axis_at), (parts,), jnp.float32, low / len(shards), high / len(shards))
        return jnp.repeat(jnp.exp(heights), dims[axis_at] // parts).reshape((-1,) + (1,) * (len(dims) - axis_at - 1))

    level = one(*shards[0])
    for cut in shards[1:]:
        level = level * one(*cut)
    return level


def shared_out(own_key, own, number, rows, count, top, reach, slope):
    ranking = jax.random.permutation(own_key, count)
    crowded, common = portions_of(count, rows * top, reach, slope, True), portions_of(count, rows * top, reach, slope, False)
    places = jnp.arange(count)

    def named(tallies, rotation):
        used = int((tallies > 0).sum())
        fixed = max(1, used // 4)
        shifted = fixed + (places - fixed + rotation * (used - fixed)) % max(1, count - fixed)
        return jnp.zeros((count,), jnp.int32).at[ranking[jnp.where(places < fixed, places, shifted)]].set(jnp.asarray(tallies, jnp.int32))

    tallies = jnp.where(number % 4 == 0, named(crowded, number // 4), named(common, number - number // 4 - 1))
    mixed = jax.random.permutation(jax.random.fold_in(own, 3), count)
    source_of, taker = mixed[0:count // 2 * 2:2], mixed[1:count // 2 * 2:2]
    room = jnp.minimum(tallies[source_of] - 1, reach - tallies[taker]) // 2
    room = jnp.where((source_of == ranking[0]) | (taker == ranking[0]) | (tallies[taker] == 0), 0, jnp.maximum(room, 0))
    shifted = jax.random.randint(jax.random.fold_in(own, 4), (count // 2,), 0, 1 << 20) % (room + 1)
    tallies = tallies.at[source_of].add(-shifted).at[taker].add(shifted)
    labels = jnp.searchsorted(jnp.cumsum(tallies), jnp.arange(rows * top), side="right").astype(jnp.int32)
    table = labels.reshape(top, rows).T
    table = table[jax.random.permutation(jax.random.fold_in(own, 1), rows)]
    rotation = jax.random.randint(jax.random.fold_in(own, 2), (rows, 1), 0, top)
    return jnp.take_along_axis(table, (jnp.arange(top)[None, :] + rotation) % top, axis=1)


def portions_of(amount, total, bound, skew, full):
    weights = [(1 << 20) // math.isqrt(standing ** skew) + 1 for standing in range(1, amount + 1)]
    largest = bound if full else min(bound, max(-(-total // amount), total * weights[0] // sum(weights)))
    least = 1 if total - largest >= amount - 1 else 0
    counts, rest = [largest] + [least] * (amount - 1), total - largest - least * (amount - 1)
    while rest > 0:
        movable = [i for i in range(1, amount) if counts[i] < largest] or [i for i in range(1, amount) if counts[i] < bound]
        mass, remaining = sum([weights[i] for i in movable]), rest
        for i in movable:
            extra = min(bound - counts[i], max(1, remaining * weights[i] // mass), rest)
            counts[i] = counts[i] + extra
            rest = rest - extra
    return np.array(counts)


def centred(rng, shape, spread, bound, cuts=(), kind=jnp.bfloat16):
    loudness = block_levels(rng, shape, cuts, -0.22, 0.18) if cuts else 1.0
    result = jax.random.normal(rng, shape, jnp.float32) * spread * loudness
    return jnp.minimum(jnp.maximum(result, -bound), bound).astype(kind)


def heavy_noise(rng, extent, width, bound, shards, heavy, kind=jnp.bfloat16):
    values = width * jax.random.normal(rng, extent, jnp.float32)
    if shards:
        values = values * block_levels(rng, extent, shards, -0.22, 0.18)
    return jnp.clip(strengthened(values, jax.random.fold_in(rng, 3), *heavy), -bound, bound).astype(kind)


def setup_inputs(seed: int = 0) -> dict:
    arg_keys = jax.random.split(jax.random.key(seed), 19)
    queries = draw_queries(jax.random.fold_in(arg_keys[18], 71), 0)
    keys = draw_keys(jax.random.fold_in(arg_keys[18], 71), 0)
    values = centred(arg_keys[2], (SEQUENCE_TOKENS, HW), 1.0, 6.0, ((0, 4), (1, 8)))
    out_gate = centred(arg_keys[3], (SEQUENCE_TOKENS, HW), 1.0, 6.0, ((0, 4), (1, 8)))
    in_gate = draw_in_gate(jax.random.fold_in(arg_keys[18], 71), 0)
    forget_gate = draw_forget_gate(jax.random.fold_in(arg_keys[18], 71), 0)
    out_gain = jnp.clip(1.0 + 0.18 * jax.random.normal(arg_keys[6], (HW,), jnp.float32), 0.1, 1.9)
    out_weight = heavy_noise(arg_keys[7], (HW, D), HW ** -0.5, 0.1875, ((0, 8),), (0, 1, 8, 2.0))
    moe_rows = draw_moe_rows(jax.random.fold_in(arg_keys[18], 71), 0)
    moe_gain = jnp.clip(1.0 + 0.18 * jax.random.normal(arg_keys[9], (D,), jnp.float32), 0.1, 1.9)
    routes_keys = jax.random.split(jax.random.fold_in(arg_keys[10], 1), TOKB // TB_DEV)
    routes_turns = jax.random.permutation(jax.random.fold_in(arg_keys[10], 3), TOKB // TB_DEV)
    routes = jax.vmap(lambda own, number: shared_out(jax.random.fold_in(arg_keys[10], 2), own, number, TB_DEV, EXPERTS, TOPK, CAP, 2))(routes_keys, routes_turns).reshape((TOKB, TOPK))
    route_weight = jnp.clip(0.2 + 1 * jax.random.uniform(arg_keys[11], (TOKB, TOPK), jnp.float32) ** block_levels(arg_keys[11], (TOKB, TOPK), ((0, 4),), -0.2, 0.2), 0.2, 1.2)
    expert_gate = centred(arg_keys[12], (EXPERTS, D, FE), D ** -0.5, 0.09375, ((0, 4), (2, 8)))
    expert_up = centred(arg_keys[13], (EXPERTS, D, FE), D ** -0.5, 0.09375, ((0, 4), (2, 8)))
    expert_down = heavy_noise(arg_keys[14], (EXPERTS, FE, D), FE ** -0.5, 0.125, ((0, 4), (1, 8)), (1, 2, 8, 2.0))
    shared_gate = centred(arg_keys[15], (D, FS), D ** -0.5, 0.09375, ((1, 8),))
    shared_up = centred(arg_keys[16], (D, FS), D ** -0.5, 0.09375, ((1, 8),))
    shared_down = heavy_noise(arg_keys[17], (FS, D), FS ** -0.5, 0.1875, ((0, 8),), (0, 1, 8, 2.0))
    return {"queries": queries, "keys": keys, "values": values, "out_gate": out_gate, "in_gate": in_gate, "forget_gate": forget_gate, "out_gain": out_gain, "out_weight": out_weight, "moe_rows": moe_rows, "moe_gain": moe_gain, "routes": routes, "route_weight": route_weight, "expert_gate": expert_gate, "expert_up": expert_up, "expert_down": expert_down, "shared_gate": shared_gate, "shared_up": shared_up, "shared_down": shared_down}


highest = lax.Precision.HIGHEST

def group_sum(left_op, right_op, groups):
    group_width = left_op.shape[1] // groups

    def add_group(group_index, running):
        first = (group_index * group_width).astype(jnp.int32)
        left_part = lax.dynamic_slice_in_dim(left_op, first, group_width, 1)
        right_part = lax.dynamic_slice_in_dim(right_op, first, group_width, 0)
        product = jnp.dot(left_part, right_part, preferred_element_type=jnp.float32)
        rounded = lax.optimization_barrier(product.astype(jnp.bfloat16))
        return running + rounded.astype(jnp.float32)
    start_sum = jnp.zeros((left_op.shape[0], right_op.shape[1]), jnp.float32)
    return lax.fori_loop(0, groups, add_group, start_sum)

def memory_head(inputs):
    query_head, key_head, value_head, gate_in, log_forget = inputs
    block_count = query_head.shape[0] // BLK
    scaled_query = (query_head * DK ** (-0.5)).reshape(block_count, BLK, DK)
    key_blocks = key_head.reshape(block_count, BLK, DK)
    value_blocks = value_head.reshape(block_count, BLK, DV)
    gate_blocks = gate_in.reshape(block_count, BLK)
    forget_blocks = log_forget.reshape(block_count, BLK)
    causal = jnp.tril(jnp.ones((BLK, BLK), dtype=bool))

    def block_step(state, block_inputs):
        matrix, normal_vec, stab = state
        query_b, key_b, value_b, gate_b, forget_b = block_inputs
        cumulative = jnp.cumsum(forget_b)
        intra = jnp.where(causal, cumulative[:, None] - cumulative[None, :] + gate_b[None, :], -jnp.inf)
        inter = cumulative + stab
        stab_t = jnp.maximum(inter, lax.optimization_barrier(jnp.max(intra, axis=1)))
        scores = jnp.dot(query_b, key_b.T, precision=highest) * jnp.exp(intra - stab_t[:, None])
        scores_low = lax.optimization_barrier(scores.astype(jnp.bfloat16)).astype(jnp.float32)
        inter_weight = jnp.exp(inter - stab_t)
        numer = jnp.dot(scores_low, value_b, precision=highest)
        numer = numer + inter_weight[:, None] * jnp.dot(query_b, matrix.T, precision=highest)
        signed = lax.optimization_barrier(jnp.sum(scores, axis=1)) + inter_weight * jnp.dot(query_b, normal_vec, precision=highest)
        cells = numer / jnp.maximum(jnp.abs(signed), jnp.exp(-stab_t))[:, None]
        block_last = cumulative[-1]
        state_logs = block_last - cumulative + gate_b
        stab_new = jnp.maximum(block_last + stab, jnp.max(state_logs))
        state_weight = jnp.exp(state_logs - stab_new)
        carried = jnp.exp(block_last + stab - stab_new)
        matrix_new = carried * matrix + jnp.dot((value_b * state_weight[:, None]).T, key_b, precision=highest)
        normal_new = carried * normal_vec + jnp.dot(state_weight, key_b, precision=highest)
        return ((matrix_new, normal_new, stab_new), cells)
    start_state = (jnp.zeros((DV, DK), jnp.float32), jnp.zeros((DK,), jnp.float32), jnp.zeros((), jnp.float32))
    _, cells = lax.scan(block_step, start_state, (scaled_query, key_blocks, value_blocks, gate_blocks, forget_blocks))
    return cells.reshape(block_count * BLK, DV)

def reference(queries, keys, values, out_gate, in_gate, forget_gate, out_gain, out_weight, moe_rows, moe_gain, routes, route_weight, expert_gate, expert_up, expert_down, shared_gate, shared_up, shared_down):
    log_forget = jax.nn.log_sigmoid(forget_gate)
    query_heads = queries.astype(jnp.float32).reshape(SEQUENCE_TOKENS, CELL_HEADS, DK).transpose(1, 0, 2)
    key_heads = keys.astype(jnp.float32).reshape(SEQUENCE_TOKENS, CELL_HEADS, DK).transpose(1, 0, 2)
    value_heads = values.astype(jnp.float32).reshape(SEQUENCE_TOKENS, CELL_HEADS, DV).transpose(1, 0, 2)
    cells = lax.map(memory_head, (query_heads, key_heads, value_heads, in_gate, log_forget))
    cells = cells.transpose(1, 0, 2).reshape(SEQUENCE_TOKENS, HW)
    mixed = (cells * jax.nn.sigmoid(out_gate.astype(jnp.float32)) * out_gain).astype(jnp.bfloat16)
    mixer_out = group_sum(mixed, out_weight, N_TP).astype(jnp.bfloat16)
    rows_wide = moe_rows.astype(jnp.float32)
    inverse = lax.rsqrt(lax.optimization_barrier(jnp.mean(rows_wide * rows_wide, axis=1, keepdims=True)) + 1e-06)
    normed = (rows_wide * inverse * moe_gain).astype(jnp.bfloat16)
    flat_routes = routes.reshape(-1).astype(jnp.int32)
    assigned = flat_routes.shape[0]
    per_block = TB_DEV * TOPK
    onehot = (flat_routes[:, None] == jnp.arange(EXPERTS, dtype=jnp.int32)[None, :]).astype(jnp.int32)
    running = jnp.cumsum(onehot.reshape(N_EP, per_block, EXPERTS), axis=1).reshape(assigned, EXPERTS)
    token_position = lax.optimization_barrier(jnp.sum(running * onehot, axis=1)) - 1
    owner_block = jnp.arange(assigned, dtype=jnp.int32) // per_block
    slot_index = (flat_routes * (N_EP * CAP) + owner_block * CAP + token_position).astype(jnp.int32)
    token_of = jnp.arange(assigned, dtype=jnp.int32) // TOPK
    slot_table = jnp.zeros((EXPERTS * N_EP * CAP,), jnp.int32).at[slot_index].set(token_of)
    slot_table = slot_table.reshape(EXPERTS, N_EP * CAP)

    def expert_rows(inputs):
        row_ids, weight_gate, weight_up, weight_down = inputs
        chosen = normed[row_ids]
        gate_val = jnp.dot(chosen, weight_gate, preferred_element_type=jnp.float32)
        up_val = jnp.dot(chosen, weight_up, preferred_element_type=jnp.float32)
        hidden = (jax.nn.silu(gate_val) * up_val).astype(jnp.bfloat16)
        return group_sum(hidden, weight_down, N_TP).astype(jnp.bfloat16)
    results = lax.map(expert_rows, (slot_table, expert_gate, expert_up, expert_down))
    picked = results.reshape(EXPERTS * N_EP * CAP, D)[slot_index].astype(jnp.float32).reshape(TOKB, TOPK, D)
    shared_gate_val = jnp.dot(normed, shared_gate, preferred_element_type=jnp.float32)
    shared_up_val = jnp.dot(normed, shared_up, preferred_element_type=jnp.float32)
    shared_hidden = (jax.nn.silu(shared_gate_val) * shared_up_val).astype(jnp.bfloat16)
    shared_sum = group_sum(shared_hidden, shared_down, N_TP)
    moe_out = (lax.optimization_barrier(jnp.sum(picked * route_weight[:, :, None], axis=1)) + shared_sum).astype(jnp.bfloat16)
    return (mixer_out, moe_out)
```

```python
import functools

import jax
import jax.numpy as jnp
from jax import lax
from jax.experimental import pallas as pl
from jax.experimental.pallas import tpu as pltpu
from jax.sharding import PartitionSpec as P

DK = 64
DV = 128
LANES = 128
SUB = 8
NEG = -1e30
EPS = 1e-06

F32 = jnp.float32
BF16 = jnp.bfloat16


def params(limit_mib=56, semantics=None):
    return pltpu.CompilerParams(vmem_limit_bytes=limit_mib << 20, dimension_semantics=semantics)


def cost(flops, nbytes, trans=0):
    return pl.CostEstimate(flops=int(flops), bytes_accessed=int(nbytes), transcendentals=int(trans))


def xor_pairs(n, k):
    return [(i, i ^ k) for i in range(n)]


def swap(x, axis, k):
    return lax.ppermute(x, axis, xor_pairs(lax.axis_size(axis), k))


def dot(a, b):
    return jnp.dot(a, b, preferred_element_type=F32)


def dot_nt(a, b):
    return lax.dot_general(a, b, (((1,), (1,)), ((), ())), preferred_element_type=F32)


def two_parts(x):
    high = x.astype(BF16)
    return high, (x - high.astype(F32)).astype(BF16)


def prep_kernel(idx, rows, gain, routes, normed, dest, *outgoing):
    n_rows, width = rows.shape
    half = width // 2
    n_out = len(outgoing)
    cap = outgoing[0].shape[0]
    topk = routes.shape[0]
    me, core = idx[0], idx[1]
    step = 16
    for first in range(0, n_rows, step):
        wide = rows[first : first + step, :].astype(F32)
        inverse = lax.rsqrt(jnp.mean(wide * wide, axis=1, keepdims=True) + EPS)
        normed[first : first + step, :] = (wide * inverse * gain[...]).astype(BF16)
    n_tgt = max(SUB, n_out)
    target = lax.broadcasted_iota(jnp.int32, (n_tgt, n_rows), 0) ^ me
    named = [routes[k : k + 1, :] == target for k in range(topk)]
    member = functools.reduce(jnp.logical_or, named)
    earlier = lax.broadcasted_iota(jnp.int32, (n_rows, n_rows), 0) < lax.broadcasted_iota(
        jnp.int32, (n_rows, n_rows), 1
    )
    place = dot(member.astype(F32).astype(BF16), earlier.astype(F32).astype(BF16)).astype(jnp.int32)
    slot = lax.broadcasted_iota(jnp.int32, (n_tgt, n_rows), 0) * cap + place
    dest[...] = jnp.zeros(dest.shape, jnp.int32)
    for k in range(topk):
        dest[k : k + 1, :] = jnp.sum(jnp.where(named[k], slot, 0), axis=0, keepdims=True)
    mine = normed[:, pl.ds(pl.multiple_of(core * half, LANES), half)]
    spot = lax.broadcasted_iota(jnp.int32, (cap, n_rows), 0)
    member_i = jnp.where(member, place, -1)
    for j in range(n_out):
        pick = (member_i[j : j + 1, :] == spot).astype(F32).astype(BF16)
        outgoing[j][...] = dot(pick, mine).astype(BF16)


def prep(idx, rows, gain, routes, n_ep, cap):
    n_rows, width = rows.shape
    shapes = [
        jax.ShapeDtypeStruct((n_rows, width), BF16),
        jax.ShapeDtypeStruct((SUB, n_rows), jnp.int32),
    ] + [jax.ShapeDtypeStruct((cap, width // 2), BF16) for _ in range(n_ep)]
    vm = pl.BlockSpec(memory_space=pltpu.VMEM)
    out = pl.pallas_call(
        prep_kernel,
        out_shape=shapes,
        in_specs=[pl.BlockSpec(memory_space=pltpu.SMEM), vm, vm, vm],
        out_specs=[vm] * len(shapes),
        compiler_params=params(),
        cost_estimate=cost(2 * n_ep * cap * n_rows * width // 2, 4 * n_rows * width),
        name="prep",
    )(idx, rows, gain, routes)
    return out[0], out[1], list(out[2:])


def ffn_kernel(idx, *refs, n_lhs, per_half, split):
    lhs, rest = refs[:n_lhs], refs[n_lhs:]
    gate, up, down, send, own, acc_g, acc_u, hidden = rest
    step = pl.program_id(0)
    n_k = 2 * per_half
    core = idx[0]

    def piece(group):
        return jnp.concatenate([r[...] for r in group], axis=0) if len(group) > 1 else group[0][...]

    def add(x):
        g = dot(x, gate[...].reshape(gate.shape[-2:]))
        u = dot(x, up[...].reshape(up.shape[-2:]))

        @pl.when(step == 0)
        def _():
            acc_g[...] = g
            acc_u[...] = u

        @pl.when(step > 0)
        def _():
            acc_g[...] += g
            acc_u[...] += u

    if split:
        n_own = n_lhs // 2

        @pl.when(step < per_half)
        def _():
            add(piece(lhs[:n_own]))

        @pl.when((step >= per_half) & (step < n_k))
        def _():
            add(piece(lhs[n_own:]))

    else:

        @pl.when(step < n_k)
        def _():
            add(piece(lhs))

    @pl.when(step == n_k - 1)
    def _():
        g = acc_g[...]
        hidden[...] = (g * jax.nn.sigmoid(g) * acc_u[...]).astype(BF16)

    @pl.when(step >= n_k)
    def _():
        y = dot(hidden[...], down[...].reshape(down.shape[-2:])).astype(BF16)
        wide = y.shape[1] // 2
        low, high = y[:, :wide], y[:, wide:]

        @pl.when(core == 0)
        def _():
            own[...] = low
            send[...] = high

        @pl.when(core != 0)
        def _():
            own[...] = high
            send[...] = low


def ffn(idx, lhs, gate, up, down, n_z, split, name):
    rows = sum(a.shape[0] for a in lhs) // (2 if split else 1)
    width, hid = gate.shape[-2:]
    chunk = 512 if split else 1024
    half = width // 2
    per_half = half // chunk
    n_k = 2 * per_half
    pair = width // n_z
    lead = gate.ndim - 2

    def k_at(j, idx):
        j = jnp.minimum(j, n_k - 1)
        if not split:
            return j
        return jnp.bitwise_xor(j // per_half, idx[0]) * per_half + j % per_half

    zeros = (0,) * lead
    ones = (1,) * lead
    if split:
        n_own = len(lhs) // 2
        lhs_specs = [
            pl.BlockSpec((a.shape[0], chunk), lambda j, idx: (0, jnp.minimum(j, per_half - 1)))
            for a in lhs[:n_own]
        ] + [
            pl.BlockSpec((a.shape[0], chunk), lambda j, idx: (0, jnp.clip(j - per_half, 0, per_half - 1)))
            for a in lhs[n_own:]
        ]
    else:
        lhs_specs = [
            pl.BlockSpec((a.shape[0], chunk), lambda j, idx: (0, jnp.minimum(j, n_k - 1))) for a in lhs
        ]
    w_in = pl.BlockSpec(ones + (chunk, hid), lambda j, idx: zeros + (k_at(j, idx), 0))
    w_out = pl.BlockSpec(ones + (hid, pair), lambda j, idx: zeros + (0, jnp.maximum(j - n_k, 0)))
    o_spec = pl.BlockSpec((rows, pair // 2), lambda j, idx: (0, jnp.maximum(j - n_k, 0)))
    shape = jax.ShapeDtypeStruct((rows, half), BF16)
    return pl.pallas_call(
        functools.partial(ffn_kernel, n_lhs=len(lhs), per_half=per_half, split=split),
        out_shape=[shape, shape],
        grid_spec=pltpu.PrefetchScalarGridSpec(
            num_scalar_prefetch=1,
            grid=(n_k + n_z,),
            in_specs=lhs_specs + [w_in, w_in, w_out],
            out_specs=[o_spec, o_spec],
            scratch_shapes=[
                pltpu.VMEM((rows, hid), F32),
                pltpu.VMEM((rows, hid), F32),
                pltpu.VMEM((rows, hid), BF16),
            ],
        ),
        compiler_params=params(semantics=("arbitrary",)),
        cost_estimate=cost(6 * rows * width * hid, 6 * width * hid + 4 * rows * width),
        name=name,
    )(idx, *lhs, gate, up, down)


def combine_kernel(idx, *refs, n_ep, topk):
    blocks, rest = refs[:n_ep], refs[n_ep:]
    shared_own, shared_other, dest, weight, out = rest
    cap = blocks[0].shape[0]
    n_rows = out.shape[1]
    back = jnp.concatenate([b[...] for b in blocks], axis=0)
    spot = lax.broadcasted_iota(jnp.int32, (n_rows, n_ep * cap), 1)
    total = shared_own[...].astype(F32) + shared_other[...].astype(F32)
    for k in range(topk):
        pick = (dest[:, k : k + 1] == spot).astype(F32).astype(BF16)
        total = total + weight[:, k : k + 1] * dot(pick, back)
    out[...] = total.astype(BF16).reshape(out.shape)


def combine(idx, blocks, shared_own, shared_other, dest, weight, n_z):
    n_rows, half = shared_own.shape
    cap = blocks[0].shape[0]
    fw = half // n_z
    topk = weight.shape[1]
    col = lambda k, idx: (0, jnp.bitwise_xor(k, idx[0]))
    keep = lambda k, idx: (0, 0)
    return pl.pallas_call(
        functools.partial(combine_kernel, n_ep=len(blocks), topk=topk),
        out_shape=jax.ShapeDtypeStruct((n_z, n_rows, fw), BF16),
        grid_spec=pltpu.PrefetchScalarGridSpec(
            num_scalar_prefetch=1,
            grid=(n_z,),
            in_specs=[pl.BlockSpec((cap, fw), col) for _ in blocks]
            + [
                pl.BlockSpec((n_rows, fw), col),
                pl.BlockSpec((n_rows, fw), col),
                pl.BlockSpec(dest.shape, keep),
                pl.BlockSpec(weight.shape, keep),
            ],
            out_specs=pl.BlockSpec((1, n_rows, fw), lambda k, idx: (k, 0, 0)),
        ),
        compiler_params=params(semantics=("arbitrary",)),
        cost_estimate=cost(2 * topk * n_rows * len(blocks) * cap * half, 4 * n_rows * half),
        name="combine",
    )(idx, *blocks, shared_own, shared_other, dest, weight)


def gate_rows(in_gate, forget_gate):
    heads, length = in_gate.shape
    head_of = lax.broadcasted_iota(jnp.int32, (SUB, length), 0) * heads // SUB
    gate = jnp.broadcast_to(in_gate[0:1, :], (SUB, length))
    forget = jnp.broadcast_to(forget_gate[0:1, :], (SUB, length))
    for h in range(1, heads):
        gate = jnp.where(head_of >= h, in_gate[h : h + 1, :], gate)
        forget = jnp.where(head_of >= h, forget_gate[h : h + 1, :], forget)
    lane = lax.broadcasted_iota(jnp.int32, (SUB, length), 1)
    cum = jnp.minimum(forget, 0.0) - jnp.log1p(jnp.exp(-jnp.abs(forget)))
    shift = 1
    while shift < length:
        cum = cum + jnp.where(lane >= shift, pltpu.roll(cum, shift, 1), 0.0)
        shift *= 2
    return gate - cum, cum, lane


def state_kernel(keys, values, in_gate, forget_gate, pack):
    heads, length = in_gate.shape
    rise, cum, _ = gate_rows(in_gate[...], forget_gate[...])
    last = cum[:, length - 1 : length]
    top = jnp.max(rise, axis=1, keepdims=True)
    weight = jnp.exp(rise - top)
    key_t = jnp.transpose(keys[...].astype(F32))
    lane = lax.broadcasted_iota(jnp.int32, (1, LANES), 1)
    pack[...] = jnp.zeros(pack.shape, F32)
    columns = []
    decay_row = jnp.zeros((1, LANES), F32)
    stab_row = jnp.zeros((1, LANES), F32)
    for h in range(heads):
        r = h * SUB // heads
        scaled = key_t[h * DK : (h + 1) * DK, :] * weight[r : r + 1, :]
        high, low = two_parts(scaled)
        v = values[:, h * DV : (h + 1) * DV]
        pack[h * DK : (h + 1) * DK, :] = dot(high, v) + dot(low, v)
        columns.append(jnp.sum(scaled, axis=1, keepdims=True))
        here = lane // DK == h
        decay_row = jnp.where(here, last[r : r + 1, :], decay_row)
        stab_row = jnp.where(here, last[r : r + 1, :] + top[r : r + 1, :], stab_row)
    if heads * DK < LANES:
        columns.append(jnp.zeros((LANES - heads * DK, 1), F32))
    column = jnp.concatenate(columns, axis=0)
    normal = jnp.transpose(jnp.broadcast_to(column, (LANES, LANES)))
    base = heads * DK
    pack[base : base + 1, :] = normal[0:1, :]
    pack[base + 1 : base + 2, :] = decay_row
    pack[base + 2 : base + 3, :] = stab_row


def cell_state(keys, values, in_gate, forget_gate):
    heads, length = in_gate.shape
    return pl.pallas_call(
        state_kernel,
        out_shape=jax.ShapeDtypeStruct((heads * DK + SUB, DV), F32),
        compiler_params=params(),
        cost_estimate=cost(4 * heads * length * DK * DV, 4 * keys.size + 2 * values.size),
        name="cell_state",
    )(keys, values, in_gate, forget_gate)


def intra_kernel(queries, keys, values, in_gate, forget_gate, inner, stats, *, block):
    heads, length = in_gate.shape
    rise, cum, lane = gate_rows(in_gate[...], forget_gate[...])
    peak = rise
    shift = 1
    while shift < length:
        peak = jnp.maximum(peak, jnp.where(lane >= shift, pltpu.roll(peak, shift, 1), NEG))
        shift *= 2
    peak_col = jnp.transpose(peak)
    cum_col = jnp.transpose(cum)
    scale = DK ** (-0.5)
    place = lax.broadcasted_iota(jnp.int32, (block, LANES), 1)
    for first in range(0, length, block):
        seen = first + block
        row = lax.broadcasted_iota(jnp.int32, (block, seen), 0) + first
        col = lax.broadcasted_iota(jnp.int32, (block, seen), 1)
        causal = col <= row
        kept = jnp.zeros((block, LANES), F32)
        for h in range(heads):
            r = h * SUB // heads
            q = queries[first:seen, h * DK : (h + 1) * DK]
            k = keys[0:seen, h * DK : (h + 1) * DK]
            v = values[0:seen, h * DV : (h + 1) * DV]
            mu = peak_col[first:seen, r : r + 1]
            decay = jnp.exp(jnp.where(causal, rise[r : r + 1, 0:seen] - mu, NEG))
            scores = dot_nt(q, k) * scale * decay
            inner[first:seen, h * DV : (h + 1) * DV] = dot(scores.astype(BF16), v)
            total = jnp.sum(scores, axis=1, keepdims=True)
            kept = jnp.where(place == 3 * h, total, kept)
            kept = jnp.where(place == 3 * h + 1, mu, kept)
            kept = jnp.where(place == 3 * h + 2, cum_col[first:seen, r : r + 1], kept)
        stats[first:seen, :] = kept


def cell_intra(queries, keys, values, in_gate, forget_gate):
    heads, length = in_gate.shape
    return pl.pallas_call(
        functools.partial(intra_kernel, block=256),
        out_shape=[
            jax.ShapeDtypeStruct((length, heads * DV), F32),
            jax.ShapeDtypeStruct((length, LANES), F32),
        ],
        compiler_params=params(),
        cost_estimate=cost(heads * length * length * (DK + DV), 8 * values.size, heads * length * length),
        name="cell_intra",
    )(queries, keys, values, in_gate, forget_gate)


def finish_kernel(idx, *refs, n_packs, heads):
    packs, rest = refs[:n_packs], refs[n_packs:]
    queries, out_gate, gain, inner, stats, mixed, high, low, small = rest
    me = idx[0]
    base = heads * DK

    @pl.when(pl.program_id(0) == 0)
    def _():
        before = [jnp.bitwise_xor(me, k + 1) for k in range(n_packs)]
        decay = [p[base + 1 : base + 2, :] for p in packs]
        after = []
        anchor = jnp.zeros((1, LANES), F32)
        for k in range(n_packs):
            gone = jnp.zeros((1, LANES), F32)
            for other in range(n_packs):
                between = (before[other] > before[k]) & (before[other] < me)
                gone = gone + jnp.where(between, decay[other], 0.0)
            after.append(gone)
            anchor = anchor + jnp.where(before[k] < me, decay[k], 0.0)
        levels = [packs[k][base + 2 : base + 3, :] + after[k] for k in range(n_packs)]
        stab = anchor
        for k in range(n_packs):
            stab = jnp.maximum(stab, jnp.where(before[k] < me, levels[k], NEG))
        weights = [
            jnp.where(before[k] < me, jnp.exp(jnp.minimum(levels[k] - stab, 0.0)), 0.0)
            for k in range(n_packs)
        ]
        normal = jnp.zeros((1, LANES), F32)
        for k in range(n_packs):
            normal = normal + weights[k] * packs[k][base : base + 1, :]
        for h in range(heads):
            matrix = jnp.zeros((DK, DV), F32)
            for k in range(n_packs):
                matrix = matrix + weights[k][:, h * DK : h * DK + 1] * packs[k][h * DK : (h + 1) * DK, :]
            a, b = two_parts(matrix)
            high[h * DK : (h + 1) * DK, :] = a
            low[h * DK : (h + 1) * DK, :] = b
        small[0:1, :] = normal
        small[1:2, :] = stab

    scale = DK ** (-0.5)
    for h in range(heads):
        cols = slice(h * DV, (h + 1) * DV)
        ks = slice(h * DK, (h + 1) * DK)
        q = queries[:, ks]
        across = (dot(q, high[ks, :]) + dot(q, low[ks, :])) * scale
        normal_dot = jnp.sum(q.astype(F32) * small[0:1, ks], axis=1, keepdims=True) * scale
        stab_in = small[1:2, h * DK : h * DK + 1]
        total = stats[:, 3 * h : 3 * h + 1]
        local_mu = stats[:, 3 * h + 1 : 3 * h + 2]
        cum = stats[:, 3 * h + 2 : 3 * h + 3]
        mu = jnp.maximum(local_mu, stab_in)
        here = jnp.exp(local_mu - mu)
        there = jnp.exp(stab_in - mu)
        signed = total * here + there * normal_dot
        divisor = jnp.maximum(jnp.abs(signed), jnp.exp(-(cum + mu)))
        cells = (inner[:, cols] * here + there * across) / divisor
        gated = cells * jax.nn.sigmoid(out_gate[:, cols].astype(F32)) * gain[:, cols]
        mixed[:, cols] = gated.astype(BF16)


def cell_finish(idx, packs, queries, out_gate, gain, inner, stats, heads):
    length, width = out_gate.shape
    block = 256
    row = lambda i, idx: (i, 0)
    keep = lambda i, idx: (0, 0)
    return pl.pallas_call(
        functools.partial(finish_kernel, n_packs=len(packs), heads=heads),
        out_shape=jax.ShapeDtypeStruct((length, width), BF16),
        grid_spec=pltpu.PrefetchScalarGridSpec(
            num_scalar_prefetch=1,
            grid=(length // block,),
            in_specs=[pl.BlockSpec(p.shape, keep) for p in packs]
            + [
                pl.BlockSpec((block, queries.shape[1]), row),
                pl.BlockSpec((block, width), row),
                pl.BlockSpec(gain.shape, keep),
                pl.BlockSpec((block, width), row),
                pl.BlockSpec((block, LANES), row),
            ],
            out_specs=pl.BlockSpec((block, width), row),
            scratch_shapes=[
                pltpu.VMEM((heads * DK, DV), BF16),
                pltpu.VMEM((heads * DK, DV), BF16),
                pltpu.VMEM((SUB, LANES), F32),
            ],
        ),
        compiler_params=params(semantics=("arbitrary",)),
        cost_estimate=cost(4 * heads * length * DK * DV, 12 * length * width, length * width),
        name="cell_finish",
    )(idx, *packs, queries, out_gate, gain, inner, stats)


def project_kernel(idx, *refs, n_tp):
    mixed, weight, out, joined = refs[:n_tp], refs[n_tp], refs[n_tp + 1], refs[n_tp + 2]
    me = idx[0]
    n_ep, _, part, _ = weight.shape
    own = n_ep * part

    @pl.when(pl.program_id(0) == 0)
    def _():
        for j in range(n_tp):
            source = jnp.bitwise_xor(me, j)
            for e in range(n_ep):
                first = j * own + e * part
                joined[first : first + part, :] = weight[e, source]

    lhs = jnp.concatenate([m[...] for m in mixed], axis=1)
    out[...] = dot(lhs, joined[...]).astype(BF16)


def project(idx, mixed, weight):
    length, own = mixed[0].shape
    n_tp = len(mixed)
    cols = weight.shape[-1]
    block = 256
    return pl.pallas_call(
        functools.partial(project_kernel, n_tp=n_tp),
        out_shape=jax.ShapeDtypeStruct((length, cols), BF16),
        grid_spec=pltpu.PrefetchScalarGridSpec(
            num_scalar_prefetch=1,
            grid=(length // block,),
            in_specs=[pl.BlockSpec((block, own), lambda i, idx: (i, 0)) for _ in mixed]
            + [pl.BlockSpec(weight.shape, lambda i, idx: (0, 0, 0, 0))],
            out_specs=pl.BlockSpec((block, cols), lambda i, idx: (i, 0)),
            scratch_shapes=[pltpu.VMEM((n_tp * own, cols), BF16)],
        ),
        compiler_params=params(semantics=("arbitrary",)),
        cost_estimate=cost(2 * length * n_tp * own * cols, 2 * length * n_tp * own),
        name="project",
    )(idx, *mixed, weight)


def local(
    queries,
    keys,
    values,
    out_gate,
    in_gate,
    forget_gate,
    out_gain,
    out_weight,
    moe_rows,
    moe_gain,
    routes,
    route_weight,
    expert_gate,
    expert_up,
    expert_down,
    shared_gate,
    shared_up,
    shared_down,
):
    n_tp, n_ep = lax.axis_size("tp"), lax.axis_size("ep")
    n_z = n_tp // 2
    me_tp, me_ep = lax.axis_index("tp"), lax.axis_index("ep")
    me_z, core = me_tp // 2, me_tp % 2
    heads = in_gate.shape[0]
    routed_rows, width = moe_rows.shape
    topk = routes.shape[1]
    exact = 3 * routed_rows * topk // (2 * n_ep)
    cap = -(-exact // 16) * 16

    idx = jnp.stack([me_ep, core]).astype(jnp.int32)
    normed, dest, outgoing = prep(
        idx, moe_rows, moe_gain.reshape(1, -1), routes.astype(jnp.int32).T, n_ep, cap
    )
    core_idx = core.reshape(1).astype(jnp.int32)
    z_idx = me_z.reshape(1).astype(jnp.int32)
    tp_idx = me_tp.reshape(1).astype(jnp.int32)
    ep_idx = me_ep.reshape(1).astype(jnp.int32)

    arrived = [outgoing[0]] + [swap(outgoing[k], "ep", k) for k in range(1, n_ep)]
    others = [swap(a, "tp", 1) for a in arrived]

    own_rows, cols = out_weight.shape
    part = own_rows // n_ep
    quarter = lax.dynamic_slice_in_dim(out_weight, me_ep * part, part, 0)
    quarter = quarter.reshape(part, n_tp, cols // n_tp).transpose(1, 0, 2)
    quarter = lax.all_to_all(quarter, "tp", 0, 0, tiled=True)
    everyone = jnp.broadcast_to(quarter[None], (n_ep,) + quarter.shape)
    columns = lax.all_to_all(everyone, "ep", 0, 0, tiled=True)

    pack = cell_state(keys, values, in_gate, forget_gate)
    packs = [swap(pack, "ep", k) for k in range(1, n_ep)]
    inner, stats = cell_intra(queries, keys, values, in_gate, forget_gate)
    shared_send, shared_own = ffn(
        core_idx, [normed], shared_gate, shared_up, shared_down, n_z, False, "shared_ffn"
    )
    shared_other = swap(shared_send, "tp", 1)
    mixed = cell_finish(
        ep_idx, packs, queries, out_gate, out_gain.reshape(1, -1), inner, stats, heads
    )
    gathered = [mixed] + [swap(mixed, "tp", 2 * k) for k in range(1, n_z)]
    pieces = []
    for g in gathered:
        pieces += [g, swap(g, "tp", 1)]

    send, own = ffn(
        core_idx, arrived + others, expert_gate, expert_up, expert_down, n_z, True, "expert_ffn"
    )
    got = swap(send, "tp", 1)
    back = []
    for k in range(n_ep):
        rows = slice(k * cap, (k + 1) * cap)
        pair = (own[rows].astype(F32) + got[rows].astype(F32)).astype(BF16)
        back.append(swap(pair, "ep", k) if k else pair)
    part_out = combine(z_idx, back, shared_own, shared_other, dest.T, route_weight, n_z)
    total = part_out[0].astype(F32)
    for k in range(1, n_z):
        total = total + swap(part_out[k], "tp", 2 * k).astype(F32)
    moe_out = total.astype(BF16)

    mixer_out = project(tp_idx, pieces, columns)
    return (mixer_out, moe_out)


def solution(mesh):
    return jax.shard_map(
        local,
        mesh=mesh,
        in_specs=(
            P("ep", "tp"),
            P("ep", "tp"),
            P("ep", "tp"),
            P("ep", "tp"),
            P("tp", "ep"),
            P("tp", "ep"),
            P("tp"),
            P("tp", None),
            P("ep", None),
            P(),
            P("ep", None),
            P("ep", None),
            P("ep", None, "tp"),
            P("ep", None, "tp"),
            P("ep", "tp", None),
            P(None, "tp"),
            P(None, "tp"),
            P("tp", None),
        ),
        out_specs=(P("ep", "tp"), P("ep", "tp")),
        check_vma=False,
    )
```

```python
import functools

import jax
import jax.numpy as jnp
from jax import lax
from jax.experimental import pallas as pl
from jax.experimental.pallas import tpu as pltpu
from jax.sharding import PartitionSpec as P


DK = 64
DV = 128
LANES = 128
SUB = 8
NEG = -1e30
EPS = 1e-06

F32 = jnp.float32
BF16 = jnp.bfloat16


def params(limit_mib=56, semantics=None):
    return pltpu.CompilerParams(vmem_limit_bytes=limit_mib << 20, dimension_semantics=semantics)


def cost(flops, nbytes, trans=0):
    return pl.CostEstimate(flops=int(flops), bytes_accessed=int(nbytes), transcendentals=int(trans))


def xor_pairs(n, k):
    return [(i, i ^ k) for i in range(n)]


def swap(x, axis, k):
    return lax.ppermute(x, axis, xor_pairs(lax.axis_size(axis), k))


def dot(a, b):
    return jnp.dot(a, b, preferred_element_type=F32)


def dot_nt(a, b):
    return lax.dot_general(a, b, (((1,), (1,)), ((), ())), preferred_element_type=F32)


def two_parts(x):
    high = x.astype(BF16)
    return high, (x - high.astype(F32)).astype(BF16)


def with_deps(kernel, n_deps, lead):
    def body(*refs):
        return kernel(*refs[:lead], *refs[lead + n_deps :])

    return body


def anywhere(deps):
    return [pl.BlockSpec(memory_space=pl.ANY) for _ in deps]


def prep_kernel(idx, rows, gain, routes, normed, dest, *outgoing):
    n_rows, width = rows.shape
    half = width // 2
    n_out = len(outgoing)
    cap = outgoing[0].shape[0]
    topk = routes.shape[0]
    me, core = idx[0], idx[1]
    step = 16
    for first in range(0, n_rows, step):
        wide = rows[first : first + step, :].astype(F32)
        inverse = lax.rsqrt(jnp.mean(wide * wide, axis=1, keepdims=True) + EPS)
        normed[first : first + step, :] = (wide * inverse * gain[...]).astype(BF16)
    n_tgt = max(SUB, n_out)
    target = lax.broadcasted_iota(jnp.int32, (n_tgt, n_rows), 0) ^ me
    named = [routes[k : k + 1, :] == target for k in range(topk)]
    member = functools.reduce(jnp.logical_or, named)
    earlier = lax.broadcasted_iota(jnp.int32, (n_rows, n_rows), 0) < lax.broadcasted_iota(
        jnp.int32, (n_rows, n_rows), 1
    )
    place = dot(member.astype(F32).astype(BF16), earlier.astype(F32).astype(BF16)).astype(jnp.int32)
    slot = lax.broadcasted_iota(jnp.int32, (n_tgt, n_rows), 0) * cap + place
    dest[...] = jnp.zeros(dest.shape, jnp.int32)
    for k in range(topk):
        dest[k : k + 1, :] = jnp.sum(jnp.where(named[k], slot, 0), axis=0, keepdims=True)
    mine = normed[:, pl.ds(pl.multiple_of(core * half, LANES), half)]
    spot = lax.broadcasted_iota(jnp.int32, (cap, n_rows), 0)
    member_i = jnp.where(member, place, -1)
    for j in range(n_out):
        pick = (member_i[j : j + 1, :] == spot).astype(F32).astype(BF16)
        outgoing[j][...] = dot(pick, mine).astype(BF16)


def prep(idx, rows, gain, routes, n_ep, cap, deps=()):
    n_rows, width = rows.shape
    shapes = [
        jax.ShapeDtypeStruct((n_rows, width), BF16),
        jax.ShapeDtypeStruct((SUB, n_rows), jnp.int32),
    ] + [jax.ShapeDtypeStruct((cap, width // 2), BF16) for _ in range(n_ep)]
    vm = pl.BlockSpec(memory_space=pltpu.VMEM)
    out = pl.pallas_call(
        with_deps(prep_kernel, len(deps), 1),
        out_shape=shapes,
        in_specs=[pl.BlockSpec(memory_space=pltpu.SMEM), *anywhere(deps), vm, vm, vm],
        out_specs=[vm] * len(shapes),
        compiler_params=params(),
        cost_estimate=cost(2 * n_ep * cap * n_rows * width // 2, 4 * n_rows * width),
        name="prep",
    )(idx, *deps, rows, gain, routes)
    return out[0], out[1], list(out[2:])


def ffn_kernel(idx, *refs, n_lhs, per_half, split):
    lhs, rest = refs[:n_lhs], refs[n_lhs:]
    gate, up, down, send, own, acc_g, acc_u, hidden = rest
    step = pl.program_id(0)
    n_k = 2 * per_half
    core = idx[0]

    def piece(group):
        return jnp.concatenate([r[...] for r in group], axis=0) if len(group) > 1 else group[0][...]

    def add(x):
        g = dot(x, gate[...].reshape(gate.shape[-2:]))
        u = dot(x, up[...].reshape(up.shape[-2:]))

        @pl.when(step == 0)
        def _():
            acc_g[...] = g
            acc_u[...] = u

        @pl.when(step > 0)
        def _():
            acc_g[...] += g
            acc_u[...] += u

    if split:
        n_own = n_lhs // 2

        @pl.when(step < per_half)
        def _():
            add(piece(lhs[:n_own]))

        @pl.when((step >= per_half) & (step < n_k))
        def _():
            add(piece(lhs[n_own:]))

    else:

        @pl.when(step < n_k)
        def _():
            add(piece(lhs))

    @pl.when(step == n_k - 1)
    def _():
        g = acc_g[...]
        hidden[...] = (g * jax.nn.sigmoid(g) * acc_u[...]).astype(BF16)

    @pl.when(step >= n_k)
    def _():
        y = dot(hidden[...], down[...].reshape(down.shape[-2:])).astype(BF16)
        wide = y.shape[1] // 2
        low, high = y[:, :wide], y[:, wide:]

        @pl.when(core == 0)
        def _():
            own[...] = low
            send[...] = high

        @pl.when(core != 0)
        def _():
            own[...] = high
            send[...] = low


def ffn(idx, lhs, gate, up, down, n_z, split, deps=()):
    rows = sum(a.shape[0] for a in lhs) // (2 if split else 1)
    width, hid = gate.shape[-2:]
    chunk = 512 if split else 1024
    half = width // 2
    per_half = half // chunk
    n_k = 2 * per_half
    pair = width // n_z
    lead = gate.ndim - 2

    def k_at(j, idx):
        j = jnp.minimum(j, n_k - 1)
        if not split:
            return j
        return jnp.bitwise_xor(j // per_half, idx[0]) * per_half + j % per_half

    zeros = (0,) * lead
    ones = (1,) * lead
    if split:
        n_own = len(lhs) // 2
        lhs_specs = [
            pl.BlockSpec((a.shape[0], chunk), lambda j, idx: (0, jnp.minimum(j, per_half - 1)))
            for a in lhs[:n_own]
        ] + [
            pl.BlockSpec((a.shape[0], chunk), lambda j, idx: (0, jnp.clip(j - per_half, 0, per_half - 1)))
            for a in lhs[n_own:]
        ]
    else:
        lhs_specs = [
            pl.BlockSpec((a.shape[0], chunk), lambda j, idx: (0, jnp.minimum(j, n_k - 1))) for a in lhs
        ]
    w_in = pl.BlockSpec(ones + (chunk, hid), lambda j, idx: zeros + (k_at(j, idx), 0))
    w_out = pl.BlockSpec(ones + (hid, pair), lambda j, idx: zeros + (0, jnp.maximum(j - n_k, 0)))
    o_spec = pl.BlockSpec((rows, pair // 2), lambda j, idx: (0, jnp.maximum(j - n_k, 0)))
    shape = jax.ShapeDtypeStruct((rows, half), BF16)
    return pl.pallas_call(
        with_deps(
            functools.partial(ffn_kernel, n_lhs=len(lhs), per_half=per_half, split=split), len(deps), 1
        ),
        out_shape=[shape, shape],
        grid_spec=pltpu.PrefetchScalarGridSpec(
            num_scalar_prefetch=1,
            grid=(n_k + n_z,),
            in_specs=anywhere(deps) + lhs_specs + [w_in, w_in, w_out],
            out_specs=[o_spec, o_spec],
            scratch_shapes=[
                pltpu.VMEM((rows, hid), F32),
                pltpu.VMEM((rows, hid), F32),
                pltpu.VMEM((rows, hid), BF16),
            ],
        ),
        compiler_params=params(semantics=("arbitrary",)),
        cost_estimate=cost(6 * rows * width * hid, 6 * width * hid + 4 * rows * width),
    )(idx, *deps, *lhs, gate, up, down)


def combine_kernel(idx, *refs, n_ep, topk):
    blocks, rest = refs[:n_ep], refs[n_ep:]
    shared_own, shared_other, dest, weight, out = rest
    cap = blocks[0].shape[0]
    n_rows = out.shape[1]
    back = jnp.concatenate([b[...] for b in blocks], axis=0)
    spot = lax.broadcasted_iota(jnp.int32, (n_rows, n_ep * cap), 1)
    total = shared_own[...].astype(F32) + shared_other[...].astype(F32)
    for k in range(topk):
        pick = (dest[:, k : k + 1] == spot).astype(F32).astype(BF16)
        total = total + weight[:, k : k + 1] * dot(pick, back)
    out[...] = total.astype(BF16).reshape(out.shape)


def combine(idx, blocks, shared_own, shared_other, dest, weight, n_z, deps=()):
    n_rows, half = shared_own.shape
    cap = blocks[0].shape[0]
    fw = half // n_z
    topk = weight.shape[1]
    col = lambda k, idx: (0, jnp.bitwise_xor(k, idx[0]))
    keep = lambda k, idx: (0, 0)
    return pl.pallas_call(
        with_deps(functools.partial(combine_kernel, n_ep=len(blocks), topk=topk), len(deps), 1),
        out_shape=jax.ShapeDtypeStruct((n_z, n_rows, fw), BF16),
        grid_spec=pltpu.PrefetchScalarGridSpec(
            num_scalar_prefetch=1,
            grid=(n_z,),
            in_specs=anywhere(deps)
            + [pl.BlockSpec((cap, fw), col) for _ in blocks]
            + [
                pl.BlockSpec((n_rows, fw), col),
                pl.BlockSpec((n_rows, fw), col),
                pl.BlockSpec(dest.shape, keep),
                pl.BlockSpec(weight.shape, keep),
            ],
            out_specs=pl.BlockSpec((1, n_rows, fw), lambda k, idx: (k, 0, 0)),
        ),
        compiler_params=params(semantics=("arbitrary",)),
        cost_estimate=cost(2 * topk * n_rows * len(blocks) * cap * half, 4 * n_rows * half),
        name="combine",
    )(idx, *deps, *blocks, shared_own, shared_other, dest, weight)


def gate_rows(in_gate, forget_gate):
    heads, length = in_gate.shape
    head_of = lax.broadcasted_iota(jnp.int32, (SUB, length), 0) * heads // SUB
    gate = jnp.broadcast_to(in_gate[0:1, :], (SUB, length))
    forget = jnp.broadcast_to(forget_gate[0:1, :], (SUB, length))
    for h in range(1, heads):
        gate = jnp.where(head_of >= h, in_gate[h : h + 1, :], gate)
        forget = jnp.where(head_of >= h, forget_gate[h : h + 1, :], forget)
    lane = lax.broadcasted_iota(jnp.int32, (SUB, length), 1)
    cum = jnp.minimum(forget, 0.0) - jnp.log1p(jnp.exp(-jnp.abs(forget)))
    shift = 1
    while shift < length:
        cum = cum + jnp.where(lane >= shift, pltpu.roll(cum, shift, 1), 0.0)
        shift *= 2
    return gate - cum, cum, lane


def state_kernel(keys, values, in_gate, forget_gate, pack):
    heads, length = in_gate.shape
    rise, cum, _ = gate_rows(in_gate[...], forget_gate[...])
    last = cum[:, length - 1 : length]
    top = jnp.max(rise, axis=1, keepdims=True)
    weight = jnp.exp(rise - top)
    key_t = jnp.transpose(keys[...].astype(F32))
    lane = lax.broadcasted_iota(jnp.int32, (1, LANES), 1)
    pack[...] = jnp.zeros(pack.shape, F32)
    columns = []
    decay_row = jnp.zeros((1, LANES), F32)
    stab_row = jnp.zeros((1, LANES), F32)
    for h in range(heads):
        r = h * SUB // heads
        scaled = key_t[h * DK : (h + 1) * DK, :] * weight[r : r + 1, :]
        high, low = two_parts(scaled)
        v = values[:, h * DV : (h + 1) * DV]
        pack[h * DK : (h + 1) * DK, :] = dot(high, v) + dot(low, v)
        columns.append(jnp.sum(scaled, axis=1, keepdims=True))
        here = lane // DK == h
        decay_row = jnp.where(here, last[r : r + 1, :], decay_row)
        stab_row = jnp.where(here, last[r : r + 1, :] + top[r : r + 1, :], stab_row)
    if heads * DK < LANES:
        columns.append(jnp.zeros((LANES - heads * DK, 1), F32))
    column = jnp.concatenate(columns, axis=0)
    normal = jnp.transpose(jnp.broadcast_to(column, (LANES, LANES)))
    base = heads * DK
    pack[base : base + 1, :] = normal[0:1, :]
    pack[base + 1 : base + 2, :] = decay_row
    pack[base + 2 : base + 3, :] = stab_row


def cell_state(keys, values, in_gate, forget_gate, deps=()):
    heads, length = in_gate.shape
    vm = pl.BlockSpec(memory_space=pltpu.VMEM)
    return pl.pallas_call(
        with_deps(state_kernel, len(deps), 0),
        in_specs=anywhere(deps) + [vm] * 4,
        out_shape=jax.ShapeDtypeStruct((heads * DK + SUB, DV), F32),
        compiler_params=params(),
        cost_estimate=cost(4 * heads * length * DK * DV, 4 * keys.size + 2 * values.size),
        name="cell_state",
    )(*deps, keys, values, in_gate, forget_gate)


def intra_kernel(queries, keys, values, in_gate, forget_gate, inner, stats, *, block):
    heads, length = in_gate.shape
    rise, cum, lane = gate_rows(in_gate[...], forget_gate[...])
    peak = rise
    shift = 1
    while shift < length:
        peak = jnp.maximum(peak, jnp.where(lane >= shift, pltpu.roll(peak, shift, 1), NEG))
        shift *= 2
    peak_col = jnp.transpose(peak)
    cum_col = jnp.transpose(cum)
    scale = DK ** (-0.5)
    place = lax.broadcasted_iota(jnp.int32, (block, LANES), 1)
    for first in range(0, length, block):
        seen = first + block
        row = lax.broadcasted_iota(jnp.int32, (block, seen), 0) + first
        col = lax.broadcasted_iota(jnp.int32, (block, seen), 1)
        causal = col <= row
        kept = jnp.zeros((block, LANES), F32)
        for h in range(heads):
            r = h * SUB // heads
            q = queries[first:seen, h * DK : (h + 1) * DK]
            k = keys[0:seen, h * DK : (h + 1) * DK]
            v = values[0:seen, h * DV : (h + 1) * DV]
            mu = peak_col[first:seen, r : r + 1]
            decay = jnp.exp(jnp.where(causal, rise[r : r + 1, 0:seen] - mu, NEG))
            scores = dot_nt(q, k) * scale * decay
            inner[first:seen, h * DV : (h + 1) * DV] = dot(scores.astype(BF16), v)
            total = jnp.sum(scores, axis=1, keepdims=True)
            kept = jnp.where(place == 3 * h, total, kept)
            kept = jnp.where(place == 3 * h + 1, mu, kept)
            kept = jnp.where(place == 3 * h + 2, cum_col[first:seen, r : r + 1], kept)
        stats[first:seen, :] = kept


def cell_intra(queries, keys, values, in_gate, forget_gate, deps=()):
    heads, length = in_gate.shape
    vm = pl.BlockSpec(memory_space=pltpu.VMEM)
    return pl.pallas_call(
        with_deps(functools.partial(intra_kernel, block=256), len(deps), 0),
        in_specs=anywhere(deps) + [vm] * 5,
        out_shape=[
            jax.ShapeDtypeStruct((length, heads * DV), F32),
            jax.ShapeDtypeStruct((length, LANES), F32),
        ],
        compiler_params=params(),
        cost_estimate=cost(heads * length * length * (DK + DV), 8 * values.size, heads * length * length),
        name="cell_intra",
    )(*deps, queries, keys, values, in_gate, forget_gate)


def finish_kernel(idx, *refs, n_packs, heads):
    packs, rest = refs[:n_packs], refs[n_packs:]
    queries, out_gate, gain, inner, stats, mixed, high, low, small = rest
    me = idx[0]
    base = heads * DK

    @pl.when(pl.program_id(0) == 0)
    def _():
        before = [jnp.bitwise_xor(me, k + 1) for k in range(n_packs)]
        decay = [p[base + 1 : base + 2, :] for p in packs]
        after = []
        anchor = jnp.zeros((1, LANES), F32)
        for k in range(n_packs):
            gone = jnp.zeros((1, LANES), F32)
            for other in range(n_packs):
                between = (before[other] > before[k]) & (before[other] < me)
                gone = gone + jnp.where(between, decay[other], 0.0)
            after.append(gone)
            anchor = anchor + jnp.where(before[k] < me, decay[k], 0.0)
        levels = [packs[k][base + 2 : base + 3, :] + after[k] for k in range(n_packs)]
        stab = anchor
        for k in range(n_packs):
            stab = jnp.maximum(stab, jnp.where(before[k] < me, levels[k], NEG))
        weights = [
            jnp.where(before[k] < me, jnp.exp(jnp.minimum(levels[k] - stab, 0.0)), 0.0)
            for k in range(n_packs)
        ]
        normal = jnp.zeros((1, LANES), F32)
        for k in range(n_packs):
            normal = normal + weights[k] * packs[k][base : base + 1, :]
        for h in range(heads):
            matrix = jnp.zeros((DK, DV), F32)
            for k in range(n_packs):
                matrix = matrix + weights[k][:, h * DK : h * DK + 1] * packs[k][h * DK : (h + 1) * DK, :]
            a, b = two_parts(matrix)
            high[h * DK : (h + 1) * DK, :] = a
            low[h * DK : (h + 1) * DK, :] = b
        small[0:1, :] = normal
        small[1:2, :] = stab

    scale = DK ** (-0.5)
    for h in range(heads):
        cols = slice(h * DV, (h + 1) * DV)
        ks = slice(h * DK, (h + 1) * DK)
        q = queries[:, ks]
        across = (dot(q, high[ks, :]) + dot(q, low[ks, :])) * scale
        normal_dot = jnp.sum(q.astype(F32) * small[0:1, ks], axis=1, keepdims=True) * scale
        stab_in = small[1:2, h * DK : h * DK + 1]
        total = stats[:, 3 * h : 3 * h + 1]
        local_mu = stats[:, 3 * h + 1 : 3 * h + 2]
        cum = stats[:, 3 * h + 2 : 3 * h + 3]
        mu = jnp.maximum(local_mu, stab_in)
        here = jnp.exp(local_mu - mu)
        there = jnp.exp(stab_in - mu)
        signed = total * here + there * normal_dot
        divisor = jnp.maximum(jnp.abs(signed), jnp.exp(-(cum + mu)))
        cells = (inner[:, cols] * here + there * across) / divisor
        gated = cells * jax.nn.sigmoid(out_gate[:, cols].astype(F32)) * gain[:, cols]
        mixed[:, cols] = gated.astype(BF16)


def cell_finish(idx, packs, queries, out_gate, gain, inner, stats, heads, deps=()):
    length, width = out_gate.shape
    block = 256
    row = lambda i, idx: (i, 0)
    keep = lambda i, idx: (0, 0)
    return pl.pallas_call(
        with_deps(functools.partial(finish_kernel, n_packs=len(packs), heads=heads), len(deps), 1),
        out_shape=jax.ShapeDtypeStruct((length, width), BF16),
        grid_spec=pltpu.PrefetchScalarGridSpec(
            num_scalar_prefetch=1,
            grid=(length // block,),
            in_specs=anywhere(deps)
            + [pl.BlockSpec(p.shape, keep) for p in packs]
            + [
                pl.BlockSpec((block, queries.shape[1]), row),
                pl.BlockSpec((block, width), row),
                pl.BlockSpec(gain.shape, keep),
                pl.BlockSpec((block, width), row),
                pl.BlockSpec((block, LANES), row),
            ],
            out_specs=pl.BlockSpec((block, width), row),
            scratch_shapes=[
                pltpu.VMEM((heads * DK, DV), BF16),
                pltpu.VMEM((heads * DK, DV), BF16),
                pltpu.VMEM((SUB, LANES), F32),
            ],
        ),
        compiler_params=params(semantics=("arbitrary",)),
        cost_estimate=cost(4 * heads * length * DK * DV, 12 * length * width, length * width),
        name="cell_finish",
    )(idx, *deps, *packs, queries, out_gate, gain, inner, stats)


def project_kernel(idx, *refs, n_tp):
    mixed, weight, out, joined = refs[:n_tp], refs[n_tp], refs[n_tp + 1], refs[n_tp + 2]
    me = idx[0]
    n_ep, _, part, _ = weight.shape
    own = n_ep * part

    @pl.when(pl.program_id(0) == 0)
    def _():
        for j in range(n_tp):
            source = jnp.bitwise_xor(me, j)
            for e in range(n_ep):
                first = j * own + e * part
                joined[first : first + part, :] = weight[e, source]

    lhs = jnp.concatenate([m[...] for m in mixed], axis=1)
    out[...] = dot(lhs, joined[...]).astype(BF16)


def project(idx, mixed, weight, deps=()):
    length, own = mixed[0].shape
    n_tp = len(mixed)
    cols = weight.shape[-1]
    block = 256
    return pl.pallas_call(
        with_deps(functools.partial(project_kernel, n_tp=n_tp), len(deps), 1),
        out_shape=jax.ShapeDtypeStruct((length, cols), BF16),
        grid_spec=pltpu.PrefetchScalarGridSpec(
            num_scalar_prefetch=1,
            grid=(length // block,),
            in_specs=anywhere(deps)
            + [pl.BlockSpec((block, own), lambda i, idx: (i, 0)) for _ in mixed]
            + [pl.BlockSpec(weight.shape, lambda i, idx: (0, 0, 0, 0))],
            out_specs=pl.BlockSpec((block, cols), lambda i, idx: (i, 0)),
            scratch_shapes=[pltpu.VMEM((n_tp * own, cols), BF16)],
        ),
        compiler_params=params(semantics=("arbitrary",)),
        cost_estimate=cost(2 * length * n_tp * own * cols, 2 * length * n_tp * own),
        name="project",
    )(idx, *deps, *mixed, weight)


def local(
    queries,
    keys,
    values,
    out_gate,
    in_gate,
    forget_gate,
    out_gain,
    out_weight,
    moe_rows,
    moe_gain,
    routes,
    route_weight,
    expert_gate,
    expert_up,
    expert_down,
    shared_gate,
    shared_up,
    shared_down,
):
    n_tp, n_ep = lax.axis_size("tp"), lax.axis_size("ep")
    n_z = n_tp // 2
    me_tp, me_ep = lax.axis_index("tp"), lax.axis_index("ep")
    me_z, core = me_tp // 2, me_tp % 2
    heads = in_gate.shape[0]
    routed_rows, _ = moe_rows.shape
    topk = routes.shape[1]
    exact = 3 * routed_rows * topk // (2 * n_ep)
    cap = -(-exact // 16) * 16

    idx = jnp.stack([me_ep, core]).astype(jnp.int32)
    core_idx = core.reshape(1).astype(jnp.int32)
    z_idx = me_z.reshape(1).astype(jnp.int32)
    tp_idx = me_tp.reshape(1).astype(jnp.int32)
    ep_idx = me_ep.reshape(1).astype(jnp.int32)

    normed, dest, outgoing = prep(
        idx, moe_rows, moe_gain.reshape(1, -1), routes.astype(jnp.int32).T, n_ep, cap
    )
    arrived = [outgoing[0]]
    for k in range(1, n_ep):
        arrived.append(swap(outgoing[k], "ep", k))

    own_rows, cols = out_weight.shape
    part = own_rows // n_ep
    share, _ = lax.optimization_barrier((out_weight, dest))
    share = lax.dynamic_slice_in_dim(share, me_ep * part, part, 0)
    share = share.reshape(part, n_tp, cols // n_tp).transpose(1, 0, 2)
    share = lax.all_to_all(share, "tp", 0, 0, tiled=True)

    pack = cell_state(keys, values, in_gate, forget_gate, [dest])
    packs = []
    for k in range(1, n_ep):
        packs.append(swap(pack, "ep", k))
    inner, stats = cell_intra(queries, keys, values, in_gate, forget_gate, [pack])
    mixed = cell_finish(
        ep_idx, packs, queries, out_gate, out_gain.reshape(1, -1), inner, stats, heads
    )
    gathered = [mixed]
    for k in range(1, n_z):
        gathered.append(swap(mixed, "tp", 2 * k))
    pieces = []
    for g in gathered:
        pieces += [g, swap(g, "tp", 1)]
    share, mixed_dep = lax.optimization_barrier((share, mixed))
    everyone = jnp.broadcast_to(share[None], (n_ep,) + share.shape)
    columns = lax.all_to_all(everyone, "ep", 0, 0, tiled=True)

    others = []
    for a in arrived:
        others.append(swap(a, "tp", 1))
    send, own = ffn(
        core_idx, arrived + others, expert_gate, expert_up, expert_down, n_z, True, [mixed_dep]
    )
    got = swap(send, "tp", 1)
    back = []
    for k in range(n_ep):
        rows = slice(k * cap, (k + 1) * cap)
        pair = (own[rows].astype(F32) + got[rows].astype(F32)).astype(BF16)
        back.append(swap(pair, "ep", k) if k else pair)
    shared_send, shared_own = ffn(
        core_idx, [normed], shared_gate, shared_up, shared_down, n_z, False, [back[0]]
    )
    shared_other = swap(shared_send, "tp", 1)
    part_out = combine(z_idx, back, shared_own, shared_other, dest.T, route_weight, n_z)
    total = part_out[0].astype(F32)
    for k in range(1, n_z):
        total = total + swap(part_out[k], "tp", 2 * k).astype(F32)
    moe_out = total.astype(BF16)
    mixer_out = project(tp_idx, pieces, columns, [part_out])
    return (mixer_out, moe_out)


def solution(mesh):
    return jax.shard_map(
        local,
        mesh=mesh,
        in_specs=(
            P("ep", "tp"),
            P("ep", "tp"),
            P("ep", "tp"),
            P("ep", "tp"),
            P("tp", "ep"),
            P("tp", "ep"),
            P("tp"),
            P("tp", None),
            P("ep", None),
            P(),
            P("ep", None),
            P("ep", None),
            P("ep", None, "tp"),
            P("ep", None, "tp"),
            P("ep", "tp", None),
            P(None, "tp"),
            P(None, "tp"),
            P("tp", None),
        ),
        out_specs=(P("ep", "tp"), P("ep", "tp")),
        check_vma=False,
    )
```

```python
import functools

import jax
import jax.numpy as jnp
from jax import lax
from jax.experimental import pallas as pl
from jax.experimental.pallas import tpu as pltpu
from jax.sharding import PartitionSpec as P


DK = 64
DV = 128
LANES = 128
SUB = 8
NEG = -1e30
EPS = 1e-06

F32 = jnp.float32
BF16 = jnp.bfloat16


def params(limit_mib=56, semantics=None):
    return pltpu.CompilerParams(vmem_limit_bytes=limit_mib << 20, dimension_semantics=semantics)


def cost(flops, nbytes, trans=0):
    return pl.CostEstimate(flops=int(flops), bytes_accessed=int(nbytes), transcendentals=int(trans))


def xor_pairs(n, k):
    return [(i, i ^ k) for i in range(n)]


def swap(x, axis, k):
    return lax.ppermute(x, axis, xor_pairs(lax.axis_size(axis), k))


def dot(a, b):
    return jnp.dot(a, b, preferred_element_type=F32)


def dot_nt(a, b):
    return lax.dot_general(a, b, (((1,), (1,)), ((), ())), preferred_element_type=F32)


def two_parts(x):
    high = x.astype(BF16)
    return high, (x - high.astype(F32)).astype(BF16)


def with_deps(kernel, n_deps, lead):
    def body(*refs):
        return kernel(*refs[:lead], *refs[lead + n_deps :])

    return body


def anywhere(deps):
    return [pl.BlockSpec(memory_space=pl.ANY) for _ in deps]


def prep_kernel(idx, rows, gain, routes, weight, normed, dest, share, *outgoing_and_sems):
    *outgoing, buf, sems = outgoing_and_sems
    n_rows, width = rows.shape
    n_tp, part, cols = share.shape
    wanted = pl.ds(pl.multiple_of(idx[2] * part, part), part)
    coming = pltpu.make_async_copy(weight.at[wanted, :], buf, sems.at[n_tp])
    coming.start()
    half = width // 2
    n_out = len(outgoing)
    cap = outgoing[0].shape[0]
    topk = routes.shape[0]
    me, core = idx[0], idx[1]
    step = 16
    for first in range(0, n_rows, step):
        wide = rows[first : first + step, :].astype(F32)
        inverse = lax.rsqrt(jnp.mean(wide * wide, axis=1, keepdims=True) + EPS)
        normed[first : first + step, :] = (wide * inverse * gain[...]).astype(BF16)
    coming.wait()
    leaving = start_all(
        [
            pltpu.make_async_copy(buf.at[:, pl.ds(t * cols, cols)], share.at[t], sems.at[t])
            for t in range(n_tp)
        ]
    )
    n_tgt = max(SUB, n_out)
    target = lax.broadcasted_iota(jnp.int32, (n_tgt, n_rows), 0) ^ me
    named = [routes[k : k + 1, :] == target for k in range(topk)]
    member = functools.reduce(jnp.logical_or, named)
    earlier = lax.broadcasted_iota(jnp.int32, (n_rows, n_rows), 0) < lax.broadcasted_iota(
        jnp.int32, (n_rows, n_rows), 1
    )
    place = dot(member.astype(F32).astype(BF16), earlier.astype(F32).astype(BF16)).astype(jnp.int32)
    slot = lax.broadcasted_iota(jnp.int32, (n_tgt, n_rows), 0) * cap + place
    dest[...] = jnp.zeros(dest.shape, jnp.int32)
    for k in range(topk):
        dest[k : k + 1, :] = jnp.sum(jnp.where(named[k], slot, 0), axis=0, keepdims=True)
    mine = normed[:, pl.ds(pl.multiple_of(core * half, LANES), half)]
    spot = lax.broadcasted_iota(jnp.int32, (cap, n_rows), 0)
    member_i = jnp.where(member, place, -1)
    for j in range(n_out):
        pick = (member_i[j : j + 1, :] == spot).astype(F32).astype(BF16)
        outgoing[j][...] = dot(pick, mine).astype(BF16)
    wait_all(leaving)


def prep(idx, rows, gain, routes, weight, n_ep, n_tp, cap, deps=()):
    n_rows, width = rows.shape
    shapes = [
        jax.ShapeDtypeStruct((n_rows, width), BF16),
        jax.ShapeDtypeStruct((SUB, n_rows), jnp.int32),
        jax.ShapeDtypeStruct((n_tp, weight.shape[0] // 2, weight.shape[1] // n_tp), BF16),
    ] + [jax.ShapeDtypeStruct((cap, width // 2), BF16) for _ in range(n_ep)]
    vm = pl.BlockSpec(memory_space=pltpu.VMEM)
    hbm = pl.BlockSpec(memory_space=pl.ANY)
    out = pl.pallas_call(
        with_deps(prep_kernel, len(deps), 1),
        out_shape=shapes,
        in_specs=[pl.BlockSpec(memory_space=pltpu.SMEM), *anywhere(deps), vm, vm, vm, hbm],
        out_specs=[vm, vm, hbm] + [vm] * n_ep,
        scratch_shapes=[
            pltpu.VMEM((weight.shape[0] // 2, weight.shape[1]), BF16),
            pltpu.SemaphoreType.DMA((n_tp + 1,)),
        ],
        compiler_params=params(),
        cost_estimate=cost(2 * n_ep * cap * n_rows * width // 2, 4 * n_rows * width),
        name="prep",
    )(idx, *deps, rows, gain, routes, weight)
    return out[0], out[1], out[2], list(out[3:])


def start_all(copies):
    for c in copies:
        c.start()
    return copies


def wait_all(copies):
    for c in copies:
        c.wait()


def gated(x, gate_buf, up_buf, arrivals, chunk):
    g = u = None
    for i, waiting in enumerate(arrivals):
        wait_all(waiting)
        rows = slice(i * chunk, (i + 1) * chunk)
        left = x[:, rows]
        g_part, u_part = dot(left, gate_buf[rows, :]), dot(left, up_buf[rows, :])
        g = g_part if g is None else g + g_part
        u = u_part if u is None else u + u_part
    return (g * jax.nn.sigmoid(g) * u).astype(BF16)


def expert_kernel(core_idx, *refs, n_ep, n_z, chunk):
    own, other, rest = refs[:n_ep], refs[n_ep : 2 * n_ep], refs[2 * n_ep :]
    gate, up, down, send, hidden, x, gate_buf, up_buf, down_buf, stage, sems = rest
    core = core_idx[0]
    cap, half = own[0].shape
    pair = down_buf.shape[1] // n_z
    count = iter(range(sems.shape[0]))

    def copy(src, dst):
        return pltpu.make_async_copy(src, dst, sems.at[next(count)])

    per_half = half // chunk
    arrivals = []
    for h, group in enumerate((own, other)):
        lhs = start_all(
            [
                copy(r, x.at[pl.ds(k * cap, cap), pl.ds(h * half, half)])
                for k, r in enumerate(group)
            ]
        )
        for i in range(per_half):
            src = pl.ds(pl.multiple_of((core ^ h) * half + i * chunk, chunk), chunk)
            dst = pl.ds(h * half + i * chunk, chunk)
            weights = start_all(
                [
                    copy(gate.at[0, src, :], gate_buf.at[dst, :]),
                    copy(up.at[0, src, :], up_buf.at[dst, :]),
                ]
            )
            arrivals.append((lhs if i == 0 else []) + weights)
    tail = start_all(
        [
            copy(
                down.at[0, :, pl.ds(pl.multiple_of((2 * n + 1 - core) * pair, LANES), pair)],
                down_buf.at[:, pl.ds(n * pair, pair)],
            )
            for n in range(n_z)
        ]
    )
    hidden[...] = gated(x, gate_buf, up_buf, arrivals, chunk)
    leaving = []
    for n in range(n_z):
        tail[n].wait()
        cols = pl.ds(n * pair, pair)
        stage[:, cols] = dot(hidden[...], down_buf[:, cols]).astype(BF16)
        leaving += start_all([copy(stage.at[:, cols], send.at[:, cols])])
    wait_all(leaving)


def expert(core_idx, own, other, gate, up, down, n_z, deps=()):
    n_ep = len(own)
    cap, half = own[0].shape
    rows = n_ep * cap
    width, hid = gate.shape[-2:]
    chunk = 512
    n_sems = 2 * n_ep + 2 * (width // chunk) + 2 * n_z
    hbm = pl.BlockSpec(memory_space=pl.ANY)
    vm = pl.BlockSpec(memory_space=pltpu.VMEM)
    return pl.pallas_call(
        with_deps(
            functools.partial(expert_kernel, n_ep=n_ep, n_z=n_z, chunk=chunk), len(deps), 1
        ),
        out_shape=[
            jax.ShapeDtypeStruct((rows, half), BF16),
            jax.ShapeDtypeStruct((rows, hid), BF16),
        ],
        in_specs=[pl.BlockSpec(memory_space=pltpu.SMEM)] + anywhere(deps) + [hbm] * (2 * n_ep + 3),
        out_specs=[hbm, vm],
        scratch_shapes=[
            pltpu.VMEM((rows, width), BF16),
            pltpu.VMEM((width, hid), BF16),
            pltpu.VMEM((width, hid), BF16),
            pltpu.VMEM((hid, half), BF16),
            pltpu.VMEM((rows, half), BF16),
            pltpu.SemaphoreType.DMA((n_sems,)),
        ],
        compiler_params=params(),
        cost_estimate=cost(5 * rows * width * hid, 5 * width * hid + 4 * rows * width),
        name="expert",
    )(core_idx, *deps, *own, *other, gate, up, down)


def pair_kernel(core_idx, hidden, got, down, *refs, n_z):
    back, down_buf, sems = refs[:-2], refs[-2], refs[-1]
    core = core_idx[0]
    cap, half = back[0].shape
    pair = half // n_z
    copies = start_all(
        [
            pltpu.make_async_copy(
                down.at[0, :, pl.ds(pl.multiple_of((2 * n + core) * pair, LANES), pair)],
                down_buf.at[:, pl.ds(n * pair, pair)],
                sems.at[n],
            )
            for n in range(n_z)
        ]
    )
    for n in range(n_z):
        copies[n].wait()
        cols = pl.ds(n * pair, pair)
        both = (dot(hidden[...], down_buf[:, cols]) + got[:, cols].astype(F32)).astype(BF16)
        for k, out in enumerate(back):
            out[:, cols] = both[k * cap : (k + 1) * cap, :]


def pair_sum(core_idx, hidden, got, down, n_ep, n_z, deps=()):
    rows, half = got.shape
    hid = hidden.shape[1]
    hbm = pl.BlockSpec(memory_space=pl.ANY)
    vm = pl.BlockSpec(memory_space=pltpu.VMEM)
    return pl.pallas_call(
        with_deps(functools.partial(pair_kernel, n_z=n_z), len(deps), 1),
        out_shape=[jax.ShapeDtypeStruct((rows // n_ep, half), BF16) for _ in range(n_ep)],
        in_specs=[pl.BlockSpec(memory_space=pltpu.SMEM)] + anywhere(deps) + [vm, vm, hbm],
        out_specs=[vm] * n_ep,
        scratch_shapes=[pltpu.VMEM((hid, half), BF16), pltpu.SemaphoreType.DMA((n_z,))],
        compiler_params=params(),
        cost_estimate=cost(2 * rows * hid * half, 2 * hid * half + 4 * rows * half),
        name="pair_sum",
    )(core_idx, *deps, hidden, got, down)


def shared_kernel(core_idx, x, gate, up, down, send, own, gate_buf, up_buf, down_buf, sems, *, n_z, chunk):
    core = core_idx[0]
    width = x.shape[1]
    pair = own.shape[1] // n_z
    count = iter(range(sems.shape[0]))

    def copy(src, dst):
        return pltpu.make_async_copy(src, dst, sems.at[next(count)])

    arrivals = []
    for i in range(width // chunk):
        rows = pl.ds(i * chunk, chunk)
        arrivals.append(
            start_all(
                [copy(gate.at[rows, :], gate_buf.at[rows, :]), copy(up.at[rows, :], up_buf.at[rows, :])]
            )
        )
    tail = start_all([copy(down, down_buf)])
    hidden = gated(x, gate_buf, up_buf, arrivals, chunk)
    wait_all(tail)
    for n in range(n_z):
        cols = pl.ds(n * pair, pair)
        for out, side in ((send, 1 - core), (own, core)):
            there = pl.ds(pl.multiple_of((2 * n + side) * pair, LANES), pair)
            out[:, cols] = dot(hidden, down_buf[:, there]).astype(BF16)


def shared(core_idx, x, gate, up, down, n_z, deps=()):
    rows, width = x.shape
    hid = gate.shape[1]
    chunk = 1024
    hbm = pl.BlockSpec(memory_space=pl.ANY)
    vm = pl.BlockSpec(memory_space=pltpu.VMEM)
    shape = jax.ShapeDtypeStruct((rows, width // 2), BF16)
    return pl.pallas_call(
        with_deps(functools.partial(shared_kernel, n_z=n_z, chunk=chunk), len(deps), 1),
        out_shape=[shape, shape],
        in_specs=[pl.BlockSpec(memory_space=pltpu.SMEM)] + anywhere(deps) + [vm, hbm, hbm, hbm],
        out_specs=[vm, vm],
        scratch_shapes=[
            pltpu.VMEM((width, hid), BF16),
            pltpu.VMEM((width, hid), BF16),
            pltpu.VMEM((hid, width), BF16),
            pltpu.SemaphoreType.DMA((2 * (width // chunk) + 1,)),
        ],
        compiler_params=params(),
        cost_estimate=cost(6 * rows * width * hid, 6 * width * hid + 4 * rows * width),
        name="shared",
    )(core_idx, *deps, x, gate, up, down)


def combine_kernel(z_idx, *refs, n_ep, n_z, topk):
    blocks, rest = refs[:n_ep], refs[n_ep:]
    shared_own, shared_other, dest, weight, outs = *rest[:4], rest[4:]
    z = z_idx[0]
    cap = blocks[0].shape[0]
    n_rows, wide = outs[0].shape
    spot = lax.broadcasted_iota(jnp.int32, (n_rows, n_ep * cap), 1)
    picks = [(dest[:, k : k + 1] == spot).astype(F32).astype(BF16) for k in range(topk)]
    shares = [jnp.broadcast_to(weight[:, k : k + 1], (n_rows, wide)) for k in range(topk)]
    for j in range(n_z):
        cols = pl.ds(pl.multiple_of((z ^ j) * wide, LANES), wide)
        back = jnp.concatenate([b[:, cols] for b in blocks], axis=0)
        total = shared_own[:, cols].astype(F32) + shared_other[:, cols].astype(F32)
        for k in range(topk):
            total = total + shares[k] * dot(picks[k], back)
        outs[j][...] = total.astype(BF16)


def combine(z_idx, blocks, shared_own, shared_other, dest, weight, n_z, deps=()):
    n_rows, half = shared_own.shape
    cap = blocks[0].shape[0]
    topk = weight.shape[1]
    vm = pl.BlockSpec(memory_space=pltpu.VMEM)
    return pl.pallas_call(
        with_deps(
            functools.partial(combine_kernel, n_ep=len(blocks), n_z=n_z, topk=topk), len(deps), 1
        ),
        out_shape=[jax.ShapeDtypeStruct((n_rows, half // n_z), BF16) for _ in range(n_z)],
        in_specs=[pl.BlockSpec(memory_space=pltpu.SMEM)]
        + anywhere(deps)
        + [vm] * (len(blocks) + 4),
        out_specs=[vm] * n_z,
        compiler_params=params(),
        cost_estimate=cost(2 * topk * n_rows * len(blocks) * cap * half, 4 * n_rows * half),
        name="combine",
    )(z_idx, *deps, *blocks, shared_own, shared_other, dest, weight)


def gate_rows(in_gate, forget_gate):
    heads, length = in_gate.shape
    head_of = lax.broadcasted_iota(jnp.int32, (SUB, length), 0) * heads // SUB
    gate = jnp.broadcast_to(in_gate[0:1, :], (SUB, length))
    forget = jnp.broadcast_to(forget_gate[0:1, :], (SUB, length))
    for h in range(1, heads):
        gate = jnp.where(head_of >= h, in_gate[h : h + 1, :], gate)
        forget = jnp.where(head_of >= h, forget_gate[h : h + 1, :], forget)
    log_forget = jnp.minimum(forget, 0.0) - jnp.log1p(jnp.exp(-jnp.abs(forget)))
    n_chunks = length // LANES
    stacked = jnp.concatenate(
        [log_forget[:, c * LANES : (c + 1) * LANES] for c in range(n_chunks)], axis=0
    )
    row = lax.broadcasted_iota(jnp.int32, (LANES, 2 * LANES), 0)
    col = lax.broadcasted_iota(jnp.int32, (LANES, 2 * LANES), 1)
    summing = ((row <= col) | (col >= LANES)).astype(F32).astype(BF16)
    first, rest = two_parts(stacked)
    second = rest
    third = ((stacked - first.astype(F32)) - second.astype(F32)).astype(BF16)
    sums = dot(first, summing) + dot(second, summing) + dot(third, summing)
    offset = jnp.zeros((SUB, LANES), F32)
    parts = []
    for c in range(n_chunks):
        rows = slice(c * SUB, (c + 1) * SUB)
        parts.append(sums[rows, :LANES] + offset)
        offset = offset + sums[rows, LANES:]
    cum = jnp.concatenate(parts, axis=1)
    return gate - cum, cum


def running_max(rise):
    length = rise.shape[1]
    n_chunks = length // LANES
    lane = lax.broadcasted_iota(jnp.int32, (n_chunks * SUB, LANES), 1)
    peak = jnp.concatenate([rise[:, c * LANES : (c + 1) * LANES] for c in range(n_chunks)], axis=0)
    shift = 1
    while shift < LANES:
        peak = jnp.maximum(peak, jnp.where(lane >= shift, pltpu.roll(peak, shift, 1), NEG))
        shift *= 2
    tops = jnp.broadcast_to(peak[:, LANES - 1 : LANES], peak.shape)
    so_far = jnp.full((SUB, LANES), NEG, F32)
    parts = []
    for c in range(n_chunks):
        rows = slice(c * SUB, (c + 1) * SUB)
        parts.append(jnp.maximum(peak[rows, :], so_far))
        so_far = jnp.maximum(so_far, tops[rows, :])
    return jnp.concatenate(parts, axis=1)


def state_kernel(keys, values, in_gate, forget_gate, pack, rows):
    heads, length = in_gate.shape
    rise, cum = gate_rows(in_gate[...], forget_gate[...])
    rows[0:SUB, :] = rise
    rows[SUB : 2 * SUB, :] = cum
    last = cum[:, length - 1 : length]
    top = jnp.max(rise, axis=1, keepdims=True)
    weight = jnp.exp(rise - top)
    key_t = jnp.transpose(keys[...].astype(F32))
    lane = lax.broadcasted_iota(jnp.int32, (1, LANES), 1)
    pack[...] = jnp.zeros(pack.shape, F32)
    columns = []
    decay_row = jnp.zeros((1, LANES), F32)
    stab_row = jnp.zeros((1, LANES), F32)
    for h in range(heads):
        r = h * SUB // heads
        scaled = key_t[h * DK : (h + 1) * DK, :] * weight[r : r + 1, :]
        high, low = two_parts(scaled)
        v = values[:, h * DV : (h + 1) * DV]
        pack[h * DK : (h + 1) * DK, :] = dot(high, v) + dot(low, v)
        columns.append(jnp.sum(scaled, axis=1, keepdims=True))
        here = lane // DK == h
        decay_row = jnp.where(here, last[r : r + 1, :], decay_row)
        stab_row = jnp.where(here, last[r : r + 1, :] + top[r : r + 1, :], stab_row)
    if heads * DK < LANES:
        columns.append(jnp.zeros((LANES - heads * DK, 1), F32))
    column = jnp.concatenate(columns, axis=0)
    normal = jnp.transpose(jnp.broadcast_to(column, (LANES, LANES)))
    base = heads * DK
    pack[base : base + 1, :] = normal[0:1, :]
    pack[base + 1 : base + 2, :] = decay_row
    pack[base + 2 : base + 3, :] = stab_row


def cell_state(keys, values, in_gate, forget_gate, deps=()):
    heads, length = in_gate.shape
    vm = pl.BlockSpec(memory_space=pltpu.VMEM)
    return pl.pallas_call(
        with_deps(state_kernel, len(deps), 0),
        in_specs=anywhere(deps) + [vm] * 4,
        out_shape=[
            jax.ShapeDtypeStruct((heads * DK + SUB, DV), F32),
            jax.ShapeDtypeStruct((2 * SUB, length), F32),
        ],
        compiler_params=params(),
        cost_estimate=cost(4 * heads * length * DK * DV, 4 * keys.size + 2 * values.size),
        name="cell_state",
    )(*deps, keys, values, in_gate, forget_gate)


def intra_kernel(queries, keys, values, rows, inner, stats, *, block, heads):
    length = queries.shape[0]
    rise = rows[0:SUB, :]
    peak = running_max(rise)
    peak_col = jnp.transpose(peak)
    scale = DK ** (-0.5)
    causal = lax.broadcasted_iota(jnp.int32, (block, block), 1) <= lax.broadcasted_iota(
        jnp.int32, (block, block), 0
    )
    place = lax.broadcasted_iota(jnp.int32, (block, SUB), 1)
    totals = []
    for first in range(0, length, block):
        seen = first + block
        kept = jnp.zeros((block, SUB), F32)
        for h in range(heads):
            r = h * SUB // heads
            ks, vs = slice(h * DK, (h + 1) * DK), slice(h * DV, (h + 1) * DV)
            q = (queries[first:seen, ks].astype(F32) * scale).astype(BF16)
            mu = peak_col[first:seen, r : r + 1]
            level = jnp.where(causal, rise[r : r + 1, first:seen] - mu, NEG)
            scores = dot_nt(q, keys[first:seen, ks]) * jnp.exp(level)
            total = jnp.sum(scores, axis=1, keepdims=True)
            part = dot(scores.astype(BF16), values[first:seen, vs])
            if first:
                scores = dot_nt(q, keys[0:first, ks]) * jnp.exp(rise[r : r + 1, 0:first] - mu)
                total = total + jnp.sum(scores, axis=1, keepdims=True)
                part = part + dot(scores.astype(BF16), values[0:first, vs])
            inner[first:seen, vs] = part
            kept = jnp.where(place * heads // SUB == h, total, kept)
        totals.append(kept)
    stats[0:SUB, :] = jnp.transpose(jnp.concatenate(totals, axis=0))
    stats[SUB : 2 * SUB, :] = peak


def cell_intra(queries, keys, values, rows, heads, deps=()):
    length = queries.shape[0]
    vm = pl.BlockSpec(memory_space=pltpu.VMEM)
    return pl.pallas_call(
        with_deps(functools.partial(intra_kernel, block=256, heads=heads), len(deps), 0),
        in_specs=anywhere(deps) + [vm] * 4,
        out_shape=[
            jax.ShapeDtypeStruct((length, heads * DV), F32),
            jax.ShapeDtypeStruct((2 * SUB, length), F32),
        ],
        compiler_params=params(),
        cost_estimate=cost(heads * length * length * (DK + DV), 8 * values.size, heads * length * length),
        name="cell_intra",
    )(*deps, queries, keys, values, rows)


def finish_kernel(ep_idx, *refs, n_packs, heads, block):
    packs, rest = refs[:n_packs], refs[n_packs:]
    queries, out_gate, gain, inner, stats, rows, mixed = rest
    me = ep_idx[0]
    base = heads * DK
    length = queries.shape[0]
    before = [jnp.bitwise_xor(me, k + 1) for k in range(n_packs)]
    decay = [p[base + 1 : base + 2, :] for p in packs]
    after = []
    anchor = jnp.zeros((1, LANES), F32)
    for k in range(n_packs):
        gone = jnp.zeros((1, LANES), F32)
        for other in range(n_packs):
            between = (before[other] > before[k]) & (before[other] < me)
            gone = gone + jnp.where(between, decay[other], 0.0)
        after.append(gone)
        anchor = anchor + jnp.where(before[k] < me, decay[k], 0.0)
    levels = [packs[k][base + 2 : base + 3, :] + after[k] for k in range(n_packs)]
    stab = anchor
    for k in range(n_packs):
        stab = jnp.maximum(stab, jnp.where(before[k] < me, levels[k], NEG))
    weights = [
        jnp.where(before[k] < me, jnp.exp(jnp.minimum(levels[k] - stab, 0.0)), 0.0)
        for k in range(n_packs)
    ]
    normal = jnp.zeros((1, LANES), F32)
    for k in range(n_packs):
        normal = normal + weights[k] * packs[k][base : base + 1, :]
    scale = DK ** (-0.5)
    total, peak, cum = stats[0:SUB, :], stats[SUB : 2 * SUB, :], rows[SUB : 2 * SUB, :]
    head_of = lax.broadcasted_iota(jnp.int32, (SUB, length), 0) * heads // SUB
    stab_in = jnp.broadcast_to(stab[:, 0:1], (SUB, length))
    normal_dot = jnp.zeros((SUB, length), F32)
    states = []
    for h in range(heads):
        ks = slice(h * DK, (h + 1) * DK)
        matrix = jnp.zeros((DK, DV), F32)
        for k in range(n_packs):
            matrix = matrix + weights[k][:, h * DK : h * DK + 1] * packs[k][ks, :]
        states.append(two_parts(matrix))
        n_high, n_low = two_parts(jnp.broadcast_to(normal[:, ks], (SUB, DK)))
        q = queries[:, ks]
        along = (dot_nt(n_high, q) + dot_nt(n_low, q)) * scale
        normal_dot = jnp.where(head_of == h, along, normal_dot)
        stab_in = jnp.where(head_of == h, stab[:, h * DK : h * DK + 1], stab_in)
    mu = jnp.maximum(peak, stab_in)
    here = jnp.exp(peak - mu)
    there = jnp.exp(stab_in - mu)
    divisor = jnp.maximum(jnp.abs(total * here + there * normal_dot), jnp.exp(-(cum + mu)))
    here_col = jnp.transpose(here / divisor)
    there_col = jnp.transpose(there / divisor * scale)
    for first in range(0, length, block):
        span = slice(first, first + block)
        for h in range(heads):
            r = h * SUB // heads
            cols, ks = slice(h * DV, (h + 1) * DV), slice(h * DK, (h + 1) * DK)
            q = queries[span, ks]
            across = dot(q, states[h][0]) + dot(q, states[h][1])
            cells = inner[span, cols] * here_col[span, r : r + 1] + across * there_col[span, r : r + 1]
            opened = jax.nn.sigmoid(out_gate[span, cols].astype(F32)) * gain[:, cols]
            mixed[span, cols] = (cells * opened).astype(BF16)


def cell_finish(ep_idx, packs, queries, out_gate, gain, inner, stats, rows, heads, deps=()):
    length, width = out_gate.shape
    vm = pl.BlockSpec(memory_space=pltpu.VMEM)
    return pl.pallas_call(
        with_deps(
            functools.partial(finish_kernel, n_packs=len(packs), heads=heads, block=256), len(deps), 1
        ),
        out_shape=jax.ShapeDtypeStruct((length, width), BF16),
        in_specs=[pl.BlockSpec(memory_space=pltpu.SMEM)]
        + anywhere(deps)
        + [vm] * (len(packs) + 6),
        compiler_params=params(),
        cost_estimate=cost(4 * heads * length * DK * DV, 12 * length * width, length * width),
        name="cell_finish",
    )(ep_idx, *deps, *packs, queries, out_gate, gain, inner, stats, rows)


def project_kernel(idx, *refs, n_tp):
    mixed, (share, low_part, high_part, out, joined, sems) = refs[:n_tp], refs[n_tp:]
    me = idx[0]
    _, part, _ = share.shape
    half_tp = n_tp // 2

    @pl.when(pl.program_id(0) == 0)
    def _():
        waits = []
        for j in range(n_tp):
            source = me ^ j
            low = source < half_tp
            bit = jnp.where(low, idx[1], idx[2])
            for h in range(2):
                first = pl.multiple_of(j * 2 * part + (bit ^ h) * part, part)
                dst, sem = joined.at[pl.ds(first, part), :], sems.at[2 * j + h]
                if h == 0:
                    pltpu.make_async_copy(share.at[source], dst, sem).start()
                else:

                    @pl.when(low)
                    def _():
                        pltpu.make_async_copy(low_part.at[source], dst, sem).start()

                    @pl.when(jnp.logical_not(low))
                    def _():
                        pltpu.make_async_copy(high_part.at[source - half_tp], dst, sem).start()

                waits.append(pltpu.make_async_copy(share.at[source], dst, sem))
        wait_all(waits)

    lhs = jnp.concatenate([m[...] for m in mixed], axis=1)
    out[...] = dot(lhs, joined[...]).astype(BF16)


def project(idx, mixed, share, low_part, high_part, deps=()):
    length, own = mixed[0].shape
    n_tp = len(mixed)
    cols = share.shape[-1]
    block = 256
    return pl.pallas_call(
        with_deps(functools.partial(project_kernel, n_tp=n_tp), len(deps), 1),
        out_shape=jax.ShapeDtypeStruct((length, cols), BF16),
        grid_spec=pltpu.PrefetchScalarGridSpec(
            num_scalar_prefetch=1,
            grid=(length // block,),
            in_specs=anywhere(deps)
            + [pl.BlockSpec((block, own), lambda i, idx: (i, 0)) for _ in mixed]
            + anywhere((share, low_part, high_part)),
            out_specs=pl.BlockSpec((block, cols), lambda i, idx: (i, 0)),
            scratch_shapes=[
                pltpu.VMEM((n_tp * own, cols), BF16),
                pltpu.SemaphoreType.DMA((2 * n_tp,)),
            ],
        ),
        compiler_params=params(semantics=("arbitrary",)),
        cost_estimate=cost(2 * length * n_tp * own * cols, 2 * length * n_tp * own),
        name="project",
    )(idx, *deps, *mixed, share, low_part, high_part)


def local(
    queries,
    keys,
    values,
    out_gate,
    in_gate,
    forget_gate,
    out_gain,
    out_weight,
    moe_rows,
    moe_gain,
    routes,
    route_weight,
    expert_gate,
    expert_up,
    expert_down,
    shared_gate,
    shared_up,
    shared_down,
):
    n_tp, n_ep = lax.axis_size("tp"), lax.axis_size("ep")
    n_z = n_tp // 2
    me_tp, me_ep = lax.axis_index("tp"), lax.axis_index("ep")
    me_z, core = me_tp // 2, me_tp % 2
    heads = in_gate.shape[0]
    routed_rows, _ = moe_rows.shape
    topk = routes.shape[1]
    exact = 3 * routed_rows * topk // (2 * n_ep)
    cap = -(-exact // 16) * 16

    low_bit, high_bit = me_ep % 2, me_ep // (n_ep // 2)
    half_tp = n_tp // 2
    own_bit = jnp.where(me_tp < half_tp, low_bit, high_bit)
    idx = jnp.stack([me_ep, core, own_bit]).astype(jnp.int32)
    core_idx = core.reshape(1).astype(jnp.int32)
    z_idx = me_z.reshape(1).astype(jnp.int32)
    ep_idx = me_ep.reshape(1).astype(jnp.int32)

    normed, dest, share, outgoing = prep(
        idx,
        moe_rows,
        moe_gain.reshape(1, -1),
        routes.astype(jnp.int32).T,
        out_weight,
        n_ep,
        n_tp,
        cap,
    )
    arrived = [outgoing[0]]
    for k in range(1, n_ep):
        arrived.append(swap(outgoing[k], "ep", k))

    share = lax.all_to_all(share, "tp", 0, 0, tiled=True)

    pack, gate_info = cell_state(keys, values, in_gate, forget_gate, [dest])
    packs = []
    for k in range(1, n_ep):
        packs.append(swap(pack, "ep", k))
    inner, stats = cell_intra(queries, keys, values, gate_info, heads, [pack])
    mixed = cell_finish(
        ep_idx, packs, queries, out_gate, out_gain.reshape(1, -1), inner, stats, gate_info, heads
    )
    gathered = [mixed]
    for k in range(1, n_z):
        gathered.append(swap(mixed, "tp", 2 * k))
    pieces = []
    for g in gathered:
        pieces += [g, swap(g, "tp", 1)]
    others = []
    for a in arrived:
        others.append(swap(a, "tp", 1))
    send, hidden = expert(
        core_idx, arrived, others, expert_gate, expert_up, expert_down, n_z, [mixed]
    )
    got = swap(send, "tp", 1)
    low_part = swap(share[:half_tp], "ep", 1)
    high_part = swap(share[half_tp:], "ep", n_ep // 2)
    sums = pair_sum(core_idx, hidden, got, expert_down, n_ep, n_z)
    back = [sums[0]]
    for k in range(1, n_ep):
        back.append(swap(sums[k], "ep", k))
    shared_send, shared_own = shared(
        core_idx, normed, shared_gate, shared_up, shared_down, n_z, [sums[0]]
    )
    shared_other = swap(shared_send, "tp", 1)
    part_out = combine(z_idx, back, shared_own, shared_other, dest.T, route_weight, n_z)
    total = part_out[0].astype(F32)
    for k in range(1, n_z):
        total = total + swap(part_out[k], "tp", 2 * k).astype(F32)
    moe_out = total.astype(BF16)
    mixer_out = project(
        jnp.stack([me_tp, low_bit, high_bit]).astype(jnp.int32), pieces, share, low_part, high_part
    )
    return (mixer_out, moe_out)


def solution(mesh):
    return jax.shard_map(
        local,
        mesh=mesh,
        in_specs=(
            P("ep", "tp"),
            P("ep", "tp"),
            P("ep", "tp"),
            P("ep", "tp"),
            P("tp", "ep"),
            P("tp", "ep"),
            P("tp"),
            P("tp", None),
            P("ep", None),
            P(),
            P("ep", None),
            P("ep", None),
            P("ep", None, "tp"),
            P("ep", None, "tp"),
            P("ep", "tp", None),
            P(None, "tp"),
            P(None, "tp"),
            P("tp", None),
        ),
        out_specs=(P("ep", "tp"), P("ep", "tp")),
        check_vma=False,
    )
```

```python
import functools

import jax
import jax.numpy as jnp
from jax import lax
from jax.experimental import pallas as pl
from jax.experimental.pallas import tpu as pltpu
from jax.sharding import PartitionSpec as P


DK = 64
DV = 128
LANES = 128
SUB = 8
NEG = -1e30
EPS = 1e-06

F32 = jnp.float32
BF16 = jnp.bfloat16


def params(limit_mib=16, semantics=None):
    return pltpu.CompilerParams(vmem_limit_bytes=limit_mib << 20, dimension_semantics=semantics)


def cost(flops, nbytes, trans=0):
    return pl.CostEstimate(flops=int(flops), bytes_accessed=int(nbytes), transcendentals=int(trans))


def xor_pairs(n, k):
    return [(i, i ^ k) for i in range(n)]


def swap(x, axis, k):
    return lax.ppermute(x, axis, xor_pairs(lax.axis_size(axis), k))


def put(xs, space):
    return [pltpu.with_memory_space_constraint(x, space) for x in xs]


def dot(a, b):
    return jnp.dot(a, b, preferred_element_type=F32)


def dot_nt(a, b):
    return lax.dot_general(a, b, (((1,), (1,)), ((), ())), preferred_element_type=F32)


def two_parts(x):
    high = x.astype(BF16)
    return high, (x - high.astype(F32)).astype(BF16)


def with_deps(kernel, n_deps, lead):
    def body(*refs):
        return kernel(*refs[:lead], *refs[lead + n_deps :])

    return body


def anywhere(deps):
    return [pl.BlockSpec(memory_space=pl.ANY) for _ in deps]


def prep_kernel(idx, rows, gain, routes, weight, normed, dest, share, *outgoing_and_sems):
    *outgoing, buf, sems = outgoing_and_sems
    n_rows, width = rows.shape
    n_tp, part, cols = share.shape
    wanted = pl.ds(pl.multiple_of(idx[2] * part, part), part)
    coming = pltpu.make_async_copy(weight.at[wanted, :], buf, sems.at[n_tp])
    coming.start()
    half = width // 2
    n_out = len(outgoing)
    cap = outgoing[0].shape[0]
    topk = routes.shape[0]
    me, core = idx[0], idx[1]
    step = 16
    for first in range(0, n_rows, step):
        wide = rows[first : first + step, :].astype(F32)
        inverse = lax.rsqrt(jnp.mean(wide * wide, axis=1, keepdims=True) + EPS)
        normed[first : first + step, :] = (wide * inverse * gain[...]).astype(BF16)
    coming.wait()
    leaving = start_all(
        [
            pltpu.make_async_copy(buf.at[:, pl.ds(t * cols, cols)], share.at[t], sems.at[t])
            for t in range(n_tp)
        ]
    )
    n_tgt = max(SUB, n_out)
    target = lax.broadcasted_iota(jnp.int32, (n_tgt, n_rows), 0) ^ me
    named = [routes[k : k + 1, :] == target for k in range(topk)]
    member = functools.reduce(jnp.logical_or, named)
    earlier = lax.broadcasted_iota(jnp.int32, (n_rows, n_rows), 0) < lax.broadcasted_iota(
        jnp.int32, (n_rows, n_rows), 1
    )
    place = dot(member.astype(F32).astype(BF16), earlier.astype(F32).astype(BF16)).astype(jnp.int32)
    slot = lax.broadcasted_iota(jnp.int32, (n_tgt, n_rows), 0) * cap + place
    dest[...] = jnp.zeros(dest.shape, jnp.int32)
    for k in range(topk):
        dest[k : k + 1, :] = jnp.sum(jnp.where(named[k], slot, 0), axis=0, keepdims=True)
    mine = normed[:, pl.ds(pl.multiple_of(core * half, LANES), half)]
    spot = lax.broadcasted_iota(jnp.int32, (cap, n_rows), 0)
    member_i = jnp.where(member, place, -1)
    for j in range(n_out):
        pick = (member_i[j : j + 1, :] == spot).astype(F32).astype(BF16)
        outgoing[j][...] = dot(pick, mine).astype(BF16)
    wait_all(leaving)


def prep(idx, rows, gain, routes, weight, n_ep, n_tp, cap, deps=()):
    n_rows, width = rows.shape
    shapes = [
        jax.ShapeDtypeStruct((n_rows, width), BF16),
        jax.ShapeDtypeStruct((SUB, n_rows), jnp.int32),
        jax.ShapeDtypeStruct((n_tp, weight.shape[0] // 2, weight.shape[1] // n_tp), BF16),
    ] + [jax.ShapeDtypeStruct((cap, width // 2), BF16) for _ in range(n_ep)]
    vm = pl.BlockSpec(memory_space=pltpu.VMEM)
    hbm = pl.BlockSpec(memory_space=pl.ANY)
    out = pl.pallas_call(
        with_deps(prep_kernel, len(deps), 1),
        out_shape=shapes,
        in_specs=[pl.BlockSpec(memory_space=pltpu.SMEM), *anywhere(deps), vm, vm, vm, hbm],
        out_specs=[vm, vm, hbm] + [vm] * n_ep,
        scratch_shapes=[
            pltpu.VMEM((weight.shape[0] // 2, weight.shape[1]), BF16),
            pltpu.SemaphoreType.DMA((n_tp + 1,)),
        ],
        compiler_params=params(),
        cost_estimate=cost(2 * n_ep * cap * n_rows * width // 2, 4 * n_rows * width),
        name="prep",
    )(idx, *deps, rows, gain, routes, weight)
    return out[0], out[1], out[2], list(out[3:])


def start_all(copies):
    for c in copies:
        c.start()
    return copies


def wait_all(copies):
    for c in copies:
        c.wait()


def gated(left_of, gate_buf, up_buf, arrivals, chunk):
    g = u = None
    for i, waiting in enumerate(arrivals):
        wait_all(waiting)
        rows = slice(i * chunk, (i + 1) * chunk)
        left = left_of(i)
        g_part, u_part = dot(left, gate_buf[rows, :]), dot(left, up_buf[rows, :])
        g = g_part if g is None else g + g_part
        u = u_part if u is None else u + u_part
    return (g * jax.nn.sigmoid(g) * u).astype(BF16)


def block_at(n, n_z, top, side, pair):
    near = n // (n_z // 2)
    block = (top ^ (1 - near)) * (n_z // 2) + n % (n_z // 2)
    return pl.ds(pl.multiple_of((2 * block + side) * pair, LANES), pair)


def expert_kernel(idx, *refs, n_ep, n_z, chunk):
    own, other, rest = refs[:n_ep], refs[n_ep : 2 * n_ep], refs[2 * n_ep :]
    gate, up, down, send_a, send_b, hidden, gate_buf, up_buf, down_buf, stage, sems = rest
    core, top = idx[0], idx[1]
    _, half = own[0].shape
    pair = down_buf.shape[1] // n_z
    count = iter(range(sems.shape[0]))

    def copy(src, dst):
        return pltpu.make_async_copy(src, dst, sems.at[next(count)])

    per_half = half // chunk
    arrivals = []
    for h in range(2):
        for i in range(per_half):
            src = pl.ds(pl.multiple_of((core ^ h) * half + i * chunk, chunk), chunk)
            dst = pl.ds(h * half + i * chunk, chunk)
            arrivals.append(
                start_all(
                    [
                        copy(gate.at[0, src, :], gate_buf.at[dst, :]),
                        copy(up.at[0, src, :], up_buf.at[dst, :]),
                    ]
                )
            )
    tail = start_all(
        [
            copy(
                down.at[0, :, block_at(n, n_z, top, 1 - core, pair)],
                down_buf.at[:, pl.ds(n * pair, pair)],
            )
            for n in range(n_z)
        ]
    )

    def rows_of(i):
        group = own if i < per_half else other
        cols = slice(i % per_half * chunk, (i % per_half + 1) * chunk)
        return jnp.concatenate([r[:, cols] for r in group], axis=0)

    hidden[...] = gated(rows_of, gate_buf, up_buf, arrivals, chunk)
    leaving = []
    for n in range(n_z):
        tail[n].wait()
        cols = pl.ds(n * pair, pair)
        stage[:, cols] = dot(hidden[...], down_buf[:, cols]).astype(BF16)
        send = (send_a, send_b)[n // (n_z // 2)]
        there = pl.ds(n % (n_z // 2) * pair, pair)
        leaving += start_all([copy(stage.at[:, cols], send.at[:, there])])
    wait_all(leaving)


def expert(core_idx, own, other, gate, up, down, n_z, deps=()):
    n_ep = len(own)
    cap, half = own[0].shape
    rows = n_ep * cap
    width, hid = gate.shape[-2:]
    chunk = 512
    n_sems = 2 * (width // chunk) + 2 * n_z
    hbm = pl.BlockSpec(memory_space=pl.ANY)
    vm = pl.BlockSpec(memory_space=pltpu.VMEM)
    return pl.pallas_call(
        with_deps(
            functools.partial(expert_kernel, n_ep=n_ep, n_z=n_z, chunk=chunk), len(deps), 1
        ),
        out_shape=[
            jax.ShapeDtypeStruct((rows, half // 2), BF16),
            jax.ShapeDtypeStruct((rows, half // 2), BF16),
            jax.ShapeDtypeStruct((rows, hid), BF16),
        ],
        in_specs=[pl.BlockSpec(memory_space=pltpu.SMEM)] + anywhere(deps) + [vm] * (2 * n_ep) + [hbm] * 3,
        out_specs=[hbm, hbm, vm],
        scratch_shapes=[
            pltpu.VMEM((width, hid), BF16),
            pltpu.VMEM((width, hid), BF16),
            pltpu.VMEM((hid, half), BF16),
            pltpu.VMEM((rows, half), BF16),
            pltpu.SemaphoreType.DMA((n_sems,)),
        ],
        compiler_params=params(36),
        cost_estimate=cost(5 * rows * width * hid, 5 * width * hid + 4 * rows * width),
        name="expert",
    )(core_idx, *deps, *own, *other, gate, up, down)


def pair_kernel(idx, hidden, got, down, *refs, n_z, part):
    back, down_buf, sems = refs[:-2], refs[-2], refs[-1]
    core, top = idx[0], idx[1]
    cap, width = back[0].shape
    n_here = n_z // 2
    pair = width // n_here
    copies = start_all(
        [
            pltpu.make_async_copy(
                down.at[0, :, block_at(part * n_here + n, n_z, top, core, pair)],
                down_buf.at[:, pl.ds(n * pair, pair)],
                sems.at[n],
            )
            for n in range(n_here)
        ]
    )
    for n in range(n_here):
        copies[n].wait()
        cols = pl.ds(n * pair, pair)
        both = (dot(hidden[...], down_buf[:, cols]) + got[:, cols].astype(F32)).astype(BF16)
        for k, out in enumerate(back):
            out[:, cols] = both[k * cap : (k + 1) * cap, :]


def pair_sum(idx, hidden, got, down, n_ep, n_z, part, deps=()):
    rows, width = got.shape
    hid = hidden.shape[1]
    hbm = pl.BlockSpec(memory_space=pl.ANY)
    vm = pl.BlockSpec(memory_space=pltpu.VMEM)
    return pl.pallas_call(
        with_deps(functools.partial(pair_kernel, n_z=n_z, part=part), len(deps), 1),
        out_shape=[jax.ShapeDtypeStruct((rows // n_ep, width), BF16) for _ in range(n_ep)],
        in_specs=[pl.BlockSpec(memory_space=pltpu.SMEM)] + anywhere(deps) + [vm, vm, hbm],
        out_specs=[vm] * n_ep,
        scratch_shapes=[pltpu.VMEM((hid, width), BF16), pltpu.SemaphoreType.DMA((n_z // 2,))],
        compiler_params=params(),
        cost_estimate=cost(2 * rows * hid * width, 2 * hid * width + 4 * rows * width),
        name="pair_sum",
    )(idx, *deps, hidden, got, down)


def shared_kernel(core_idx, x, gate, up, down, send, own, gate_buf, up_buf, down_buf, sems, *, n_z, chunk):
    core = core_idx[0]
    width = x.shape[1]
    pair = own.shape[1] // n_z
    count = iter(range(sems.shape[0]))

    def copy(src, dst):
        return pltpu.make_async_copy(src, dst, sems.at[next(count)])

    arrivals = []
    for i in range(width // chunk):
        rows = pl.ds(i * chunk, chunk)
        arrivals.append(
            start_all(
                [copy(gate.at[rows, :], gate_buf.at[rows, :]), copy(up.at[rows, :], up_buf.at[rows, :])]
            )
        )
    tail = start_all([copy(down, down_buf)])
    hidden = gated(
        lambda i: x[:, i * chunk : (i + 1) * chunk], gate_buf, up_buf, arrivals, chunk
    )
    wait_all(tail)
    for n in range(n_z):
        cols = pl.ds(n * pair, pair)
        for out, side in ((send, 1 - core), (own, core)):
            there = pl.ds(pl.multiple_of((2 * n + side) * pair, LANES), pair)
            out[:, cols] = dot(hidden, down_buf[:, there]).astype(BF16)


def shared(core_idx, x, gate, up, down, n_z, deps=()):
    rows, width = x.shape
    hid = gate.shape[1]
    chunk = 1024
    hbm = pl.BlockSpec(memory_space=pl.ANY)
    vm = pl.BlockSpec(memory_space=pltpu.VMEM)
    shape = jax.ShapeDtypeStruct((rows, width // 2), BF16)
    return pl.pallas_call(
        with_deps(functools.partial(shared_kernel, n_z=n_z, chunk=chunk), len(deps), 1),
        out_shape=[shape, shape],
        in_specs=[pl.BlockSpec(memory_space=pltpu.SMEM)] + anywhere(deps) + [vm, hbm, hbm, hbm],
        out_specs=[vm, vm],
        scratch_shapes=[
            pltpu.VMEM((width, hid), BF16),
            pltpu.VMEM((width, hid), BF16),
            pltpu.VMEM((hid, width), BF16),
            pltpu.SemaphoreType.DMA((2 * (width // chunk) + 1,)),
        ],
        compiler_params=params(24),
        cost_estimate=cost(6 * rows * width * hid, 6 * width * hid + 4 * rows * width),
        name="shared",
    )(core_idx, *deps, x, gate, up, down)


def combine_kernel(z_idx, *refs, n_ep, n_z, topk, part):
    blocks, rest = refs[:n_ep], refs[n_ep:]
    shared_own, shared_other, dest, weight, outs = *rest[:4], rest[4:]
    z = z_idx[0]
    cap = blocks[0].shape[0]
    n_rows, wide = outs[0].shape
    n_here = n_z // 2
    spot = lax.broadcasted_iota(jnp.int32, (n_rows, n_ep * cap), 1)
    picks = [(dest[:, k : k + 1] == spot).astype(F32).astype(BF16) for k in range(topk)]
    shares = [jnp.broadcast_to(weight[:, k : k + 1], (n_rows, wide)) for k in range(topk)]
    for j in range(n_here):
        block = z ^ (j if part else j + n_here)
        there = pl.ds(pl.multiple_of((block & (n_here - 1)) * wide, LANES), wide)
        cols = pl.ds(pl.multiple_of(block * wide, LANES), wide)
        back = jnp.concatenate([b[:, there] for b in blocks], axis=0)
        total = shared_own[:, cols].astype(F32) + shared_other[:, cols].astype(F32)
        for k in range(topk):
            total = total + shares[k] * dot(picks[k], back)
        outs[j][...] = total.astype(BF16)


def combine(z_idx, blocks, shared_own, shared_other, dest, weight, n_z, part, deps=()):
    n_rows, half = shared_own.shape
    cap = blocks[0].shape[0]
    topk = weight.shape[1]
    n_here = n_z // 2
    vm = pl.BlockSpec(memory_space=pltpu.VMEM)
    return pl.pallas_call(
        with_deps(
            functools.partial(combine_kernel, n_ep=len(blocks), n_z=n_z, topk=topk, part=part),
            len(deps),
            1,
        ),
        out_shape=[jax.ShapeDtypeStruct((n_rows, half // n_z), BF16) for _ in range(n_here)],
        in_specs=[pl.BlockSpec(memory_space=pltpu.SMEM)]
        + anywhere(deps)
        + [vm] * (len(blocks) + 4),
        out_specs=[vm] * n_here,
        compiler_params=params(),
        cost_estimate=cost(topk * n_rows * len(blocks) * cap * half, 2 * n_rows * half),
        name="combine",
    )(z_idx, *deps, *blocks, shared_own, shared_other, dest, weight)


def gate_rows(in_gate, forget_gate):
    heads, length = in_gate.shape
    head_of = lax.broadcasted_iota(jnp.int32, (SUB, length), 0) * heads // SUB
    gate = jnp.broadcast_to(in_gate[0:1, :], (SUB, length))
    forget = jnp.broadcast_to(forget_gate[0:1, :], (SUB, length))
    for h in range(1, heads):
        gate = jnp.where(head_of >= h, in_gate[h : h + 1, :], gate)
        forget = jnp.where(head_of >= h, forget_gate[h : h + 1, :], forget)
    log_forget = jnp.minimum(forget, 0.0) - jnp.log1p(jnp.exp(-jnp.abs(forget)))
    n_chunks = length // LANES
    stacked = jnp.concatenate(
        [log_forget[:, c * LANES : (c + 1) * LANES] for c in range(n_chunks)], axis=0
    )
    row = lax.broadcasted_iota(jnp.int32, (LANES, 2 * LANES), 0)
    col = lax.broadcasted_iota(jnp.int32, (LANES, 2 * LANES), 1)
    summing = ((row <= col) | (col >= LANES)).astype(F32).astype(BF16)
    first, rest = two_parts(stacked)
    second = rest
    third = ((stacked - first.astype(F32)) - second.astype(F32)).astype(BF16)
    sums = dot(first, summing) + dot(second, summing) + dot(third, summing)
    offset = jnp.zeros((SUB, LANES), F32)
    parts = []
    for c in range(n_chunks):
        rows = slice(c * SUB, (c + 1) * SUB)
        parts.append(sums[rows, :LANES] + offset)
        offset = offset + sums[rows, LANES:]
    cum = jnp.concatenate(parts, axis=1)
    return gate - cum, cum


def running_max(rise):
    length = rise.shape[1]
    n_chunks = length // LANES
    lane = lax.broadcasted_iota(jnp.int32, (n_chunks * SUB, LANES), 1)
    peak = jnp.concatenate([rise[:, c * LANES : (c + 1) * LANES] for c in range(n_chunks)], axis=0)
    shift = 1
    while shift < LANES:
        peak = jnp.maximum(peak, jnp.where(lane >= shift, pltpu.roll(peak, shift, 1), NEG))
        shift *= 2
    tops = jnp.broadcast_to(peak[:, LANES - 1 : LANES], peak.shape)
    so_far = jnp.full((SUB, LANES), NEG, F32)
    parts = []
    for c in range(n_chunks):
        rows = slice(c * SUB, (c + 1) * SUB)
        parts.append(jnp.maximum(peak[rows, :], so_far))
        so_far = jnp.maximum(so_far, tops[rows, :])
    return jnp.concatenate(parts, axis=1)


def state_kernel(keys, values, in_gate, forget_gate, pack, rows):
    heads, length = in_gate.shape
    rise, cum = gate_rows(in_gate[...], forget_gate[...])
    rows[0:SUB, :] = rise
    rows[SUB : 2 * SUB, :] = cum
    last = cum[:, length - 1 : length]
    top = jnp.max(rise, axis=1, keepdims=True)
    weight = jnp.exp(rise - top)
    key_t = jnp.transpose(keys[...].astype(F32))
    lane = lax.broadcasted_iota(jnp.int32, (1, LANES), 1)
    pack[...] = jnp.zeros(pack.shape, F32)
    columns = []
    decay_row = jnp.zeros((1, LANES), F32)
    stab_row = jnp.zeros((1, LANES), F32)
    for h in range(heads):
        r = h * SUB // heads
        scaled = key_t[h * DK : (h + 1) * DK, :] * weight[r : r + 1, :]
        high, low = two_parts(scaled)
        v = values[:, h * DV : (h + 1) * DV]
        pack[h * DK : (h + 1) * DK, :] = dot(high, v) + dot(low, v)
        columns.append(jnp.sum(scaled, axis=1, keepdims=True))
        here = lane // DK == h
        decay_row = jnp.where(here, last[r : r + 1, :], decay_row)
        stab_row = jnp.where(here, last[r : r + 1, :] + top[r : r + 1, :], stab_row)
    if heads * DK < LANES:
        columns.append(jnp.zeros((LANES - heads * DK, 1), F32))
    column = jnp.concatenate(columns, axis=0)
    normal = jnp.transpose(jnp.broadcast_to(column, (LANES, LANES)))
    base = heads * DK
    pack[base : base + 1, :] = normal[0:1, :]
    pack[base + 1 : base + 2, :] = decay_row
    pack[base + 2 : base + 3, :] = stab_row


def cell_state(keys, values, in_gate, forget_gate, deps=()):
    heads, length = in_gate.shape
    vm = pl.BlockSpec(memory_space=pltpu.VMEM)
    return pl.pallas_call(
        with_deps(state_kernel, len(deps), 0),
        in_specs=anywhere(deps) + [vm] * 4,
        out_shape=[
            jax.ShapeDtypeStruct((heads * DK + SUB, DV), F32),
            jax.ShapeDtypeStruct((2 * SUB, length), F32),
        ],
        compiler_params=params(),
        cost_estimate=cost(4 * heads * length * DK * DV, 4 * keys.size + 2 * values.size),
        name="cell_state",
    )(*deps, keys, values, in_gate, forget_gate)


def intra_kernel(queries, keys, values, rows, inner, stats, *, block, heads):
    length = queries.shape[0]
    rise = rows[0:SUB, :]
    peak = running_max(rise)
    peak_col = jnp.transpose(peak)
    scale = DK ** (-0.5)
    causal = lax.broadcasted_iota(jnp.int32, (block, block), 1) <= lax.broadcasted_iota(
        jnp.int32, (block, block), 0
    )
    place = lax.broadcasted_iota(jnp.int32, (block, SUB), 1)
    totals = []
    for first in range(0, length, block):
        seen = first + block
        kept = jnp.zeros((block, SUB), F32)
        for h in range(heads):
            r = h * SUB // heads
            ks, vs = slice(h * DK, (h + 1) * DK), slice(h * DV, (h + 1) * DV)
            q = (queries[first:seen, ks].astype(F32) * scale).astype(BF16)
            mu = peak_col[first:seen, r : r + 1]
            level = jnp.where(causal, rise[r : r + 1, first:seen] - mu, NEG)
            scores = dot_nt(q, keys[first:seen, ks]) * jnp.exp(level)
            total = jnp.sum(scores, axis=1, keepdims=True)
            part = dot(scores.astype(BF16), values[first:seen, vs])
            if first:
                scores = dot_nt(q, keys[0:first, ks]) * jnp.exp(rise[r : r + 1, 0:first] - mu)
                total = total + jnp.sum(scores, axis=1, keepdims=True)
                part = part + dot(scores.astype(BF16), values[0:first, vs])
            inner[first:seen, vs] = part
            kept = jnp.where(place * heads // SUB == h, total, kept)
        totals.append(kept)
    stats[0:SUB, :] = jnp.transpose(jnp.concatenate(totals, axis=0))
    stats[SUB : 2 * SUB, :] = peak


def cell_intra(queries, keys, values, rows, heads, deps=()):
    length = queries.shape[0]
    vm = pl.BlockSpec(memory_space=pltpu.VMEM)
    return pl.pallas_call(
        with_deps(functools.partial(intra_kernel, block=256, heads=heads), len(deps), 0),
        in_specs=anywhere(deps) + [vm] * 4,
        out_shape=[
            jax.ShapeDtypeStruct((length, heads * DV), F32),
            jax.ShapeDtypeStruct((2 * SUB, length), F32),
        ],
        compiler_params=params(),
        cost_estimate=cost(heads * length * length * (DK + DV), 8 * values.size, heads * length * length),
        name="cell_intra",
    )(*deps, queries, keys, values, rows)


def finish_kernel(ep_idx, *refs, n_packs, heads, block):
    packs, rest = refs[:n_packs], refs[n_packs:]
    queries, out_gate, gain, inner, stats, rows, mixed = rest
    me = ep_idx[0]
    base = heads * DK
    length = queries.shape[0]
    before = [jnp.bitwise_xor(me, k + 1) for k in range(n_packs)]
    decay = [p[base + 1 : base + 2, :] for p in packs]
    after = []
    anchor = jnp.zeros((1, LANES), F32)
    for k in range(n_packs):
        gone = jnp.zeros((1, LANES), F32)
        for other in range(n_packs):
            between = (before[other] > before[k]) & (before[other] < me)
            gone = gone + jnp.where(between, decay[other], 0.0)
        after.append(gone)
        anchor = anchor + jnp.where(before[k] < me, decay[k], 0.0)
    levels = [packs[k][base + 2 : base + 3, :] + after[k] for k in range(n_packs)]
    stab = anchor
    for k in range(n_packs):
        stab = jnp.maximum(stab, jnp.where(before[k] < me, levels[k], NEG))
    weights = [
        jnp.where(before[k] < me, jnp.exp(jnp.minimum(levels[k] - stab, 0.0)), 0.0)
        for k in range(n_packs)
    ]
    normal = jnp.zeros((1, LANES), F32)
    for k in range(n_packs):
        normal = normal + weights[k] * packs[k][base : base + 1, :]
    scale = DK ** (-0.5)
    total, peak, cum = stats[0:SUB, :], stats[SUB : 2 * SUB, :], rows[SUB : 2 * SUB, :]
    head_of = lax.broadcasted_iota(jnp.int32, (SUB, length), 0) * heads // SUB
    stab_in = jnp.broadcast_to(stab[:, 0:1], (SUB, length))
    normal_dot = jnp.zeros((SUB, length), F32)
    states = []
    for h in range(heads):
        ks = slice(h * DK, (h + 1) * DK)
        matrix = jnp.zeros((DK, DV), F32)
        for k in range(n_packs):
            matrix = matrix + weights[k][:, h * DK : h * DK + 1] * packs[k][ks, :]
        states.append(two_parts(matrix))
        n_high, n_low = two_parts(jnp.broadcast_to(normal[:, ks], (SUB, DK)))
        q = queries[:, ks]
        along = (dot_nt(n_high, q) + dot_nt(n_low, q)) * scale
        normal_dot = jnp.where(head_of == h, along, normal_dot)
        stab_in = jnp.where(head_of == h, stab[:, h * DK : h * DK + 1], stab_in)
    mu = jnp.maximum(peak, stab_in)
    here = jnp.exp(peak - mu)
    there = jnp.exp(stab_in - mu)
    divisor = jnp.maximum(jnp.abs(total * here + there * normal_dot), jnp.exp(-(cum + mu)))
    here_col = jnp.transpose(here / divisor)
    there_col = jnp.transpose(there / divisor * scale)
    for first in range(0, length, block):
        span = slice(first, first + block)
        for h in range(heads):
            r = h * SUB // heads
            cols, ks = slice(h * DV, (h + 1) * DV), slice(h * DK, (h + 1) * DK)
            q = queries[span, ks]
            across = dot(q, states[h][0]) + dot(q, states[h][1])
            cells = inner[span, cols] * here_col[span, r : r + 1] + across * there_col[span, r : r + 1]
            opened = jax.nn.sigmoid(out_gate[span, cols].astype(F32)) * gain[:, cols]
            mixed[span, cols] = (cells * opened).astype(BF16)


def cell_finish(ep_idx, packs, queries, out_gate, gain, inner, stats, rows, heads, deps=()):
    length, width = out_gate.shape
    vm = pl.BlockSpec(memory_space=pltpu.VMEM)
    return pl.pallas_call(
        with_deps(
            functools.partial(finish_kernel, n_packs=len(packs), heads=heads, block=256), len(deps), 1
        ),
        out_shape=jax.ShapeDtypeStruct((length, width), BF16),
        in_specs=[pl.BlockSpec(memory_space=pltpu.SMEM)]
        + anywhere(deps)
        + [vm] * (len(packs) + 6),
        compiler_params=params(),
        cost_estimate=cost(4 * heads * length * DK * DV, 12 * length * width, length * width),
        name="cell_finish",
    )(ep_idx, *deps, *packs, queries, out_gate, gain, inner, stats, rows)


def project_kernel(idx, *refs, n_tp, block):
    mixed, rest = refs[:n_tp], refs[n_tp:]
    share, low_part, high_part, out, joined, stage, sems = rest
    me = idx[0]
    _, part, _ = share.shape
    length = mixed[0].shape[0]
    half_tp = n_tp // 2
    for j in range(n_tp):
        source = me ^ j
        low = source < half_tp
        bit = jnp.where(low, idx[1], idx[2])
        first = j * 2 * part
        here = pl.ds(pl.multiple_of(first + bit * part, part), part)
        there = pl.ds(pl.multiple_of(first + (bit ^ 1) * part, part), part)
        joined[here, :] = share[source]

        @pl.when(low)
        def _():
            joined[there, :] = low_part[source]

        @pl.when(jnp.logical_not(low))
        def _():
            joined[there, :] = high_part[source - half_tp]

    leaving = []
    for b in range(length // block):
        rows = slice(b * block, (b + 1) * block)
        lhs = jnp.concatenate([m[rows, :] for m in mixed], axis=1)
        stage[rows, :] = dot(lhs, joined[...]).astype(BF16)
        span = pl.ds(b * block, block)
        leaving += start_all(
            [pltpu.make_async_copy(stage.at[span, :], out.at[span, :], sems.at[b])]
        )
    wait_all(leaving)


def project(idx, mixed, share, low_part, high_part, deps=()):
    length, own = mixed[0].shape
    n_tp = len(mixed)
    cols = share.shape[-1]
    block = 256
    hbm = pl.BlockSpec(memory_space=pl.ANY)
    vm = pl.BlockSpec(memory_space=pltpu.VMEM)
    return pl.pallas_call(
        with_deps(functools.partial(project_kernel, n_tp=n_tp, block=block), len(deps), 1),
        out_shape=jax.ShapeDtypeStruct((length, cols), BF16),
        in_specs=[pl.BlockSpec(memory_space=pltpu.SMEM)] + anywhere(deps) + [vm] * (n_tp + 3),
        out_specs=hbm,
        scratch_shapes=[
            pltpu.VMEM((n_tp * own, cols), BF16),
            pltpu.VMEM((length, cols), BF16),
            pltpu.SemaphoreType.DMA((length // block,)),
        ],
        compiler_params=params(20),
        cost_estimate=cost(2 * length * n_tp * own * cols, 2 * length * n_tp * own),
        name="project",
    )(idx, *deps, *mixed, share, low_part, high_part)


def local(
    queries,
    keys,
    values,
    out_gate,
    in_gate,
    forget_gate,
    out_gain,
    out_weight,
    moe_rows,
    moe_gain,
    routes,
    route_weight,
    expert_gate,
    expert_up,
    expert_down,
    shared_gate,
    shared_up,
    shared_down,
):
    n_tp, n_ep = lax.axis_size("tp"), lax.axis_size("ep")
    n_z = n_tp // 2
    me_tp, me_ep = lax.axis_index("tp"), lax.axis_index("ep")
    me_z, core = me_tp // 2, me_tp % 2
    heads = in_gate.shape[0]
    routed_rows, _ = moe_rows.shape
    topk = routes.shape[1]
    exact = 3 * routed_rows * topk // (2 * n_ep)
    cap = -(-exact // 16) * 16

    low_bit, high_bit = me_ep % 2, me_ep // (n_ep // 2)
    half_tp = n_tp // 2
    own_bit = jnp.where(me_tp < half_tp, low_bit, high_bit)
    idx = jnp.stack([me_ep, core, own_bit]).astype(jnp.int32)
    core_idx = core.reshape(1).astype(jnp.int32)
    z_idx = me_z.reshape(1).astype(jnp.int32)
    ep_idx = me_ep.reshape(1).astype(jnp.int32)

    normed, dest, share, outgoing = prep(
        idx,
        *put([moe_rows], pltpu.HBM),
        moe_gain.reshape(1, -1),
        routes.astype(jnp.int32).T,
        *put([out_weight], pltpu.HBM),
        n_ep,
        n_tp,
        cap,
    )
    arrived = [outgoing[0]]
    for k in range(1, n_ep):
        arrived.append(swap(outgoing[k], "ep", k))

    share = lax.all_to_all(share, "tp", 0, 0, tiled=True)

    pack, gate_info = cell_state(keys, values, in_gate, forget_gate, [dest])
    packs = []
    for k in range(1, n_ep):
        packs.append(swap(pack, "ep", k))
    inner, stats = cell_intra(queries, keys, values, gate_info, heads, [pack])
    mixed = cell_finish(
        ep_idx, put(packs, pltpu.VMEM), queries, out_gate, out_gain.reshape(1, -1), inner, stats, gate_info, heads
    )
    gathered = [mixed]
    for k in range(1, n_z):
        gathered.append(swap(mixed, "tp", 2 * k))
    pieces = []
    for g in gathered:
        pieces += [g, swap(g, "tp", 1)]
    others = []
    for a in arrived:
        others.append(swap(a, "tp", 1))
    dest_cols = dest.T
    weight_cols = route_weight * jnp.ones((1, 1), F32)
    project_idx = jnp.stack([me_tp, low_bit, high_bit]).astype(jnp.int32)
    half_idx = jnp.stack([core, me_z // (n_z // 2)]).astype(jnp.int32)
    *sends, hidden = expert(
        half_idx, put(arrived, pltpu.VMEM), put(others, pltpu.VMEM), *put([expert_gate, expert_up, expert_down], pltpu.HBM), n_z, [mixed]
    )
    got = []
    for part in range(2):
        got.append(swap(sends[part], "tp", 1))
    backs, dep = [], hidden
    for part in range(2):
        sums = pair_sum(
            half_idx, hidden, *put([got[part]], pltpu.VMEM), *put([expert_down], pltpu.HBM), n_ep, n_z, part, [dep]
        )
        dep = sums[0]
        back = [sums[0]]
        for k in range(1, n_ep):
            back.append(swap(sums[k], "ep", k))
        backs.append(back)
    low_part = swap(share[:half_tp], "ep", 1)
    high_part = swap(share[half_tp:], "ep", n_ep // 2)
    shared_send, shared_own = shared(
        core_idx,
        normed,
        *put([shared_gate, shared_up, shared_down], pltpu.HBM),
        n_z,
        [dep, dest_cols, weight_cols, project_idx],
    )
    shared_other = swap(shared_send, "tp", 1)
    parts, total, dep = [None] * n_z, None, shared_own
    for part in range(2):
        outs = combine(
            z_idx, put(backs[part], pltpu.VMEM), shared_own, *put([shared_other], pltpu.VMEM), dest_cols, weight_cols, n_z, part, [dep]
        )
        dep = outs[0]
        first = 0 if part else n_z // 2
        parts[first : first + n_z // 2] = outs
    total = parts[0].astype(F32)
    for k in range(1, n_z):
        total = total + swap(parts[k], "tp", 2 * k).astype(F32)
    moe_out = total.astype(BF16)
    mixer_out = project(
        project_idx, put(pieces, pltpu.VMEM), *put([share, low_part, high_part], pltpu.VMEM), [dep]
    )
    return (mixer_out, moe_out)


def solution(mesh):
    return jax.shard_map(
        local,
        mesh=mesh,
        in_specs=(
            P("ep", "tp"),
            P("ep", "tp"),
            P("ep", "tp"),
            P("ep", "tp"),
            P("tp", "ep"),
            P("tp", "ep"),
            P("tp"),
            P("tp", None),
            P("ep", None),
            P(),
            P("ep", None),
            P("ep", None),
            P("ep", None, "tp"),
            P("ep", None, "tp"),
            P("ep", "tp", None),
            P(None, "tp"),
            P(None, "tp"),
            P("tp", None),
        ),
        out_specs=(P("ep", "tp"), P("ep", "tp")),
        check_vma=False,
    )
```

```python
import functools

import jax
import jax.numpy as jnp
from jax import lax
from jax.experimental import pallas as pl
from jax.experimental.pallas import tpu as pltpu
from jax.sharding import PartitionSpec as P


DK = 64
DV = 128
LANES = 128
SUB = 8
NEG = -1e30
EPS = 1e-06

F32 = jnp.float32
BF16 = jnp.bfloat16


def params(limit_mib=16, semantics=None):
    return pltpu.CompilerParams(vmem_limit_bytes=limit_mib << 20, dimension_semantics=semantics)


def cost(flops, nbytes, trans=0):
    return pl.CostEstimate(flops=int(flops), bytes_accessed=int(nbytes), transcendentals=int(trans))


def xor_pairs(n, k):
    return [(i, i ^ k) for i in range(n)]


def swap(x, axis, k):
    return lax.ppermute(x, axis, xor_pairs(lax.axis_size(axis), k))


def put(xs, space):
    return [pltpu.with_memory_space_constraint(x, space) for x in xs]


def dot(a, b):
    return jnp.dot(a, b, preferred_element_type=F32)


def dot_nt(a, b):
    return lax.dot_general(a, b, (((1,), (1,)), ((), ())), preferred_element_type=F32)


def two_parts(x):
    high = x.astype(BF16)
    return high, (x - high.astype(F32)).astype(BF16)


def with_deps(kernel, n_deps, lead):
    def body(*refs):
        return kernel(*refs[:lead], *refs[lead + n_deps :])

    return body


def anywhere(deps):
    return [pl.BlockSpec(memory_space=pl.ANY) for _ in deps]


def prep_kernel(idx, rows, gain, routes, weight, normed, dest, share, *outgoing_and_sems):
    *outgoing, buf, sems = outgoing_and_sems
    n_rows, width = rows.shape
    n_tp, part, cols = share.shape
    wanted = pl.ds(pl.multiple_of(idx[2] * part, part), part)
    coming = pltpu.make_async_copy(weight.at[wanted, :], buf, sems.at[n_tp])
    coming.start()
    half = width // 2
    n_out = len(outgoing)
    cap = outgoing[0].shape[0]
    topk = routes.shape[0]
    me, core = idx[0], idx[1]
    step = 16
    for first in range(0, n_rows, step):
        wide = rows[first : first + step, :].astype(F32)
        inverse = lax.rsqrt(jnp.mean(wide * wide, axis=1, keepdims=True) + EPS)
        normed[first : first + step, :] = (wide * inverse * gain[...]).astype(BF16)
    coming.wait()
    leaving = start_all(
        [
            pltpu.make_async_copy(buf.at[:, pl.ds(t * cols, cols)], share.at[t], sems.at[t])
            for t in range(n_tp)
        ]
    )
    n_tgt = max(SUB, n_out)
    target = lax.broadcasted_iota(jnp.int32, (n_tgt, n_rows), 0) ^ me
    named = [routes[k : k + 1, :] == target for k in range(topk)]
    member = functools.reduce(jnp.logical_or, named)
    earlier = lax.broadcasted_iota(jnp.int32, (n_rows, n_rows), 0) < lax.broadcasted_iota(
        jnp.int32, (n_rows, n_rows), 1
    )
    place = dot(member.astype(F32).astype(BF16), earlier.astype(F32).astype(BF16)).astype(jnp.int32)
    slot = lax.broadcasted_iota(jnp.int32, (n_tgt, n_rows), 0) * cap + place
    dest[...] = jnp.zeros(dest.shape, jnp.int32)
    for k in range(topk):
        dest[k : k + 1, :] = jnp.sum(jnp.where(named[k], slot, 0), axis=0, keepdims=True)
    mine = normed[:, pl.ds(pl.multiple_of(core * half, LANES), half)]
    spot = lax.broadcasted_iota(jnp.int32, (cap, n_rows), 0)
    member_i = jnp.where(member, place, -1)
    for j in range(n_out):
        pick = (member_i[j : j + 1, :] == spot).astype(F32).astype(BF16)
        outgoing[j][...] = dot(pick, mine).astype(BF16)
    wait_all(leaving)


def prep(idx, rows, gain, routes, weight, n_ep, n_tp, cap, deps=()):
    n_rows, width = rows.shape
    shapes = [
        jax.ShapeDtypeStruct((n_rows, width), BF16),
        jax.ShapeDtypeStruct((SUB, n_rows), jnp.int32),
        jax.ShapeDtypeStruct((n_tp, weight.shape[0] // 2, weight.shape[1] // n_tp), BF16),
    ] + [jax.ShapeDtypeStruct((cap, width // 2), BF16) for _ in range(n_ep)]
    vm = pl.BlockSpec(memory_space=pltpu.VMEM)
    hbm = pl.BlockSpec(memory_space=pl.ANY)
    out = pl.pallas_call(
        with_deps(prep_kernel, len(deps), 1),
        out_shape=shapes,
        in_specs=[pl.BlockSpec(memory_space=pltpu.SMEM), *anywhere(deps), vm, vm, vm, hbm],
        out_specs=[vm, vm, hbm] + [vm] * n_ep,
        scratch_shapes=[
            pltpu.VMEM((weight.shape[0] // 2, weight.shape[1]), BF16),
            pltpu.SemaphoreType.DMA((n_tp + 1,)),
        ],
        compiler_params=params(),
        cost_estimate=cost(2 * n_ep * cap * n_rows * width // 2, 4 * n_rows * width),
        name="prep",
    )(idx, *deps, rows, gain, routes, weight)
    return out[0], out[1], out[2], list(out[3:])


def start_all(copies):
    for c in copies:
        c.start()
    return copies


def wait_all(copies):
    for c in copies:
        c.wait()


def gated(left_of, gate_buf, up_buf, arrivals, chunk):
    g = u = None
    for i, waiting in enumerate(arrivals):
        wait_all(waiting)
        rows = slice(i * chunk, (i + 1) * chunk)
        left = left_of(i)
        g_part, u_part = dot(left, gate_buf[rows, :]), dot(left, up_buf[rows, :])
        g = g_part if g is None else g + g_part
        u = u_part if u is None else u + u_part
    return (g * jax.nn.sigmoid(g) * u).astype(BF16)


def block_at(n, n_z, top, side, pair):
    near = n // (n_z // 2)
    block = (top ^ (1 - near)) * (n_z // 2) + n % (n_z // 2)
    return pl.ds(pl.multiple_of((2 * block + side) * pair, LANES), pair)


def expert_kernel(idx, *refs, n_ep, n_z, chunk):
    own, other, rest = refs[:n_ep], refs[n_ep : 2 * n_ep], refs[2 * n_ep :]
    gate, up, down, send_a, send_b, hidden, gate_buf, up_buf, down_buf, stage, sems = rest
    core, top = idx[0], idx[1]
    _, half = own[0].shape
    pair = down_buf.shape[1] // n_z
    count = iter(range(sems.shape[0]))

    def copy(src, dst):
        return pltpu.make_async_copy(src, dst, sems.at[next(count)])

    per_half = half // chunk
    arrivals = []
    for h in range(2):
        for i in range(per_half):
            src = pl.ds(pl.multiple_of((core ^ h) * half + i * chunk, chunk), chunk)
            dst = pl.ds(h * half + i * chunk, chunk)
            arrivals.append(
                start_all(
                    [
                        copy(gate.at[0, src, :], gate_buf.at[dst, :]),
                        copy(up.at[0, src, :], up_buf.at[dst, :]),
                    ]
                )
            )
    tail = start_all(
        [
            copy(
                down.at[0, :, block_at(n, n_z, top, 1 - core, pair)],
                down_buf.at[:, pl.ds(n * pair, pair)],
            )
            for n in range(n_z)
        ]
    )

    def rows_of(i):
        group = own if i < per_half else other
        cols = slice(i % per_half * chunk, (i % per_half + 1) * chunk)
        return jnp.concatenate([r[:, cols] for r in group], axis=0)

    hidden[...] = gated(rows_of, gate_buf, up_buf, arrivals, chunk)
    leaving = []
    for n in range(n_z):
        tail[n].wait()
        cols = pl.ds(n * pair, pair)
        stage[:, cols] = dot(hidden[...], down_buf[:, cols]).astype(BF16)
        send = (send_a, send_b)[n // (n_z // 2)]
        there = pl.ds(n % (n_z // 2) * pair, pair)
        leaving += start_all([copy(stage.at[:, cols], send.at[:, there])])
    wait_all(leaving)


def expert(core_idx, own, other, gate, up, down, n_z, deps=()):
    n_ep = len(own)
    cap, half = own[0].shape
    rows = n_ep * cap
    width, hid = gate.shape[-2:]
    chunk = 512
    n_sems = 2 * (width // chunk) + 2 * n_z
    hbm = pl.BlockSpec(memory_space=pl.ANY)
    vm = pl.BlockSpec(memory_space=pltpu.VMEM)
    return pl.pallas_call(
        with_deps(
            functools.partial(expert_kernel, n_ep=n_ep, n_z=n_z, chunk=chunk), len(deps), 1
        ),
        out_shape=[
            jax.ShapeDtypeStruct((rows, half // 2), BF16),
            jax.ShapeDtypeStruct((rows, half // 2), BF16),
            jax.ShapeDtypeStruct((rows, hid), BF16),
        ],
        in_specs=[pl.BlockSpec(memory_space=pltpu.SMEM)] + anywhere(deps) + [vm] * (2 * n_ep) + [hbm] * 3,
        out_specs=[hbm, hbm, vm],
        scratch_shapes=[
            pltpu.VMEM((width, hid), BF16),
            pltpu.VMEM((width, hid), BF16),
            pltpu.VMEM((hid, half), BF16),
            pltpu.VMEM((rows, half), BF16),
            pltpu.SemaphoreType.DMA((n_sems,)),
        ],
        compiler_params=params(36),
        cost_estimate=cost(5 * rows * width * hid, 5 * width * hid + 4 * rows * width),
        name="expert",
    )(core_idx, *deps, *own, *other, gate, up, down)


def pair_kernel(idx, hidden, got, down, *refs, n_z, part):
    back, down_buf, sems = refs[:-2], refs[-2], refs[-1]
    core, top = idx[0], idx[1]
    cap, width = back[0].shape
    n_here = n_z // 2
    pair = width // n_here
    copies = start_all(
        [
            pltpu.make_async_copy(
                down.at[0, :, block_at(part * n_here + n, n_z, top, core, pair)],
                down_buf.at[:, pl.ds(n * pair, pair)],
                sems.at[n],
            )
            for n in range(n_here)
        ]
    )
    for n in range(n_here):
        copies[n].wait()
        cols = pl.ds(n * pair, pair)
        both = (dot(hidden[...], down_buf[:, cols]) + got[:, cols].astype(F32)).astype(BF16)
        for k, out in enumerate(back):
            out[:, cols] = both[k * cap : (k + 1) * cap, :]


def pair_sum(idx, hidden, got, down, n_ep, n_z, part, deps=()):
    rows, width = got.shape
    hid = hidden.shape[1]
    hbm = pl.BlockSpec(memory_space=pl.ANY)
    vm = pl.BlockSpec(memory_space=pltpu.VMEM)
    return pl.pallas_call(
        with_deps(functools.partial(pair_kernel, n_z=n_z, part=part), len(deps), 1),
        out_shape=[jax.ShapeDtypeStruct((rows // n_ep, width), BF16) for _ in range(n_ep)],
        in_specs=[pl.BlockSpec(memory_space=pltpu.SMEM)] + anywhere(deps) + [vm, vm, hbm],
        out_specs=[vm] * n_ep,
        scratch_shapes=[pltpu.VMEM((hid, width), BF16), pltpu.SemaphoreType.DMA((n_z // 2,))],
        compiler_params=params(),
        cost_estimate=cost(2 * rows * hid * width, 2 * hid * width + 4 * rows * width),
        name="pair_sum",
    )(idx, *deps, hidden, got, down)


def shared_kernel(core_idx, x, gate, up, down, send, own, gate_buf, up_buf, down_buf, sems, *, n_z, chunk):
    core = core_idx[0]
    width = x.shape[1]
    pair = own.shape[1] // n_z
    count = iter(range(sems.shape[0]))

    def copy(src, dst):
        return pltpu.make_async_copy(src, dst, sems.at[next(count)])

    arrivals = []
    for i in range(width // chunk):
        rows = pl.ds(i * chunk, chunk)
        arrivals.append(
            start_all(
                [copy(gate.at[rows, :], gate_buf.at[rows, :]), copy(up.at[rows, :], up_buf.at[rows, :])]
            )
        )
    tail = start_all([copy(down, down_buf)])
    hidden = gated(
        lambda i: x[:, i * chunk : (i + 1) * chunk], gate_buf, up_buf, arrivals, chunk
    )
    wait_all(tail)
    for n in range(n_z):
        cols = pl.ds(n * pair, pair)
        for out, side in ((send, 1 - core), (own, core)):
            there = pl.ds(pl.multiple_of((2 * n + side) * pair, LANES), pair)
            out[:, cols] = dot(hidden, down_buf[:, there]).astype(BF16)


def shared(core_idx, x, gate, up, down, n_z, deps=()):
    rows, width = x.shape
    hid = gate.shape[1]
    chunk = 1024
    hbm = pl.BlockSpec(memory_space=pl.ANY)
    vm = pl.BlockSpec(memory_space=pltpu.VMEM)
    shape = jax.ShapeDtypeStruct((rows, width // 2), BF16)
    return pl.pallas_call(
        with_deps(functools.partial(shared_kernel, n_z=n_z, chunk=chunk), len(deps), 1),
        out_shape=[shape, shape],
        in_specs=[pl.BlockSpec(memory_space=pltpu.SMEM)] + anywhere(deps) + [vm, hbm, hbm, hbm],
        out_specs=[vm, vm],
        scratch_shapes=[
            pltpu.VMEM((width, hid), BF16),
            pltpu.VMEM((width, hid), BF16),
            pltpu.VMEM((hid, width), BF16),
            pltpu.SemaphoreType.DMA((2 * (width // chunk) + 1,)),
        ],
        compiler_params=params(24),
        cost_estimate=cost(6 * rows * width * hid, 6 * width * hid + 4 * rows * width),
        name="shared",
    )(core_idx, *deps, x, gate, up, down)


def combine_kernel(z_idx, *refs, n_ep, n_z, topk, part):
    blocks, rest = refs[:n_ep], refs[n_ep:]
    shared_own, shared_other, dest, weight, outs = *rest[:4], rest[4:]
    z = z_idx[0]
    cap = blocks[0].shape[0]
    n_rows, wide = outs[0].shape
    n_here = n_z // 2
    spot = lax.broadcasted_iota(jnp.int32, (n_rows, n_ep * cap), 1)
    picks = [(dest[:, k : k + 1] == spot).astype(F32).astype(BF16) for k in range(topk)]
    shares = [jnp.broadcast_to(weight[:, k : k + 1], (n_rows, wide)) for k in range(topk)]
    for j in range(n_here):
        block = z ^ (j if part else j + n_here)
        there = pl.ds(pl.multiple_of((block & (n_here - 1)) * wide, LANES), wide)
        cols = pl.ds(pl.multiple_of(block * wide, LANES), wide)
        back = jnp.concatenate([b[:, there] for b in blocks], axis=0)
        total = shared_own[:, cols].astype(F32) + shared_other[:, cols].astype(F32)
        for k in range(topk):
            total = total + shares[k] * dot(picks[k], back)
        outs[j][...] = total.astype(BF16)


def combine(z_idx, blocks, shared_own, shared_other, dest, weight, n_z, part, deps=()):
    n_rows, half = shared_own.shape
    cap = blocks[0].shape[0]
    topk = weight.shape[1]
    n_here = n_z // 2
    vm = pl.BlockSpec(memory_space=pltpu.VMEM)
    return pl.pallas_call(
        with_deps(
            functools.partial(combine_kernel, n_ep=len(blocks), n_z=n_z, topk=topk, part=part),
            len(deps),
            1,
        ),
        out_shape=[jax.ShapeDtypeStruct((n_rows, half // n_z), BF16) for _ in range(n_here)],
        in_specs=[pl.BlockSpec(memory_space=pltpu.SMEM)]
        + anywhere(deps)
        + [vm] * (len(blocks) + 4),
        out_specs=[vm] * n_here,
        compiler_params=params(),
        cost_estimate=cost(topk * n_rows * len(blocks) * cap * half, 2 * n_rows * half),
        name="combine",
    )(z_idx, *deps, *blocks, shared_own, shared_other, dest, weight)


def gate_rows(in_gate, forget_gate):
    heads, length = in_gate.shape
    head_of = lax.broadcasted_iota(jnp.int32, (SUB, length), 0) * heads // SUB
    gate = jnp.broadcast_to(in_gate[0:1, :], (SUB, length))
    forget = jnp.broadcast_to(forget_gate[0:1, :], (SUB, length))
    for h in range(1, heads):
        gate = jnp.where(head_of >= h, in_gate[h : h + 1, :], gate)
        forget = jnp.where(head_of >= h, forget_gate[h : h + 1, :], forget)
    log_forget = jnp.minimum(forget, 0.0) - jnp.log1p(jnp.exp(-jnp.abs(forget)))
    n_chunks = length // LANES
    stacked = jnp.concatenate(
        [log_forget[:, c * LANES : (c + 1) * LANES] for c in range(n_chunks)], axis=0
    )
    row = lax.broadcasted_iota(jnp.int32, (LANES, 2 * LANES), 0)
    col = lax.broadcasted_iota(jnp.int32, (LANES, 2 * LANES), 1)
    summing = ((row <= col) | (col >= LANES)).astype(F32).astype(BF16)
    first, rest = two_parts(stacked)
    second = rest
    third = ((stacked - first.astype(F32)) - second.astype(F32)).astype(BF16)
    sums = dot(first, summing) + dot(second, summing) + dot(third, summing)
    offset = jnp.zeros((SUB, LANES), F32)
    parts = []
    for c in range(n_chunks):
        rows = slice(c * SUB, (c + 1) * SUB)
        parts.append(sums[rows, :LANES] + offset)
        offset = offset + sums[rows, LANES:]
    cum = jnp.concatenate(parts, axis=1)
    return gate - cum, cum


def running_max(rise):
    length = rise.shape[1]
    n_chunks = length // LANES
    lane = lax.broadcasted_iota(jnp.int32, (n_chunks * SUB, LANES), 1)
    peak = jnp.concatenate([rise[:, c * LANES : (c + 1) * LANES] for c in range(n_chunks)], axis=0)
    shift = 1
    while shift < LANES:
        peak = jnp.maximum(peak, jnp.where(lane >= shift, pltpu.roll(peak, shift, 1), NEG))
        shift *= 2
    tops = jnp.broadcast_to(peak[:, LANES - 1 : LANES], peak.shape)
    so_far = jnp.full((SUB, LANES), NEG, F32)
    parts = []
    for c in range(n_chunks):
        rows = slice(c * SUB, (c + 1) * SUB)
        parts.append(jnp.maximum(peak[rows, :], so_far))
        so_far = jnp.maximum(so_far, tops[rows, :])
    return jnp.concatenate(parts, axis=1)


def state_kernel(keys, values, in_gate, forget_gate, pack, rows):
    heads, length = in_gate.shape
    rise, cum = gate_rows(in_gate[...], forget_gate[...])
    rows[0:SUB, :] = rise
    rows[SUB : 2 * SUB, :] = cum
    last = cum[:, length - 1 : length]
    top = jnp.max(rise, axis=1, keepdims=True)
    weight = jnp.exp(rise - top)
    key_t = jnp.transpose(keys[...].astype(F32))
    lane = lax.broadcasted_iota(jnp.int32, (1, LANES), 1)
    pack[...] = jnp.zeros(pack.shape, F32)
    columns = []
    decay_row = jnp.zeros((1, LANES), F32)
    stab_row = jnp.zeros((1, LANES), F32)
    for h in range(heads):
        r = h * SUB // heads
        scaled = key_t[h * DK : (h + 1) * DK, :] * weight[r : r + 1, :]
        high, low = two_parts(scaled)
        v = values[:, h * DV : (h + 1) * DV]
        pack[h * DK : (h + 1) * DK, :] = dot(high, v) + dot(low, v)
        columns.append(jnp.sum(scaled, axis=1, keepdims=True))
        here = lane // DK == h
        decay_row = jnp.where(here, last[r : r + 1, :], decay_row)
        stab_row = jnp.where(here, last[r : r + 1, :] + top[r : r + 1, :], stab_row)
    if heads * DK < LANES:
        columns.append(jnp.zeros((LANES - heads * DK, 1), F32))
    column = jnp.concatenate(columns, axis=0)
    normal = jnp.transpose(jnp.broadcast_to(column, (LANES, LANES)))
    base = heads * DK
    pack[base : base + 1, :] = normal[0:1, :]
    pack[base + 1 : base + 2, :] = decay_row
    pack[base + 2 : base + 3, :] = stab_row


def cell_state(keys, values, in_gate, forget_gate, deps=()):
    heads, length = in_gate.shape
    vm = pl.BlockSpec(memory_space=pltpu.VMEM)
    return pl.pallas_call(
        with_deps(state_kernel, len(deps), 0),
        in_specs=anywhere(deps) + [vm] * 4,
        out_shape=[
            jax.ShapeDtypeStruct((heads * DK + SUB, DV), F32),
            jax.ShapeDtypeStruct((2 * SUB, length), F32),
        ],
        compiler_params=params(),
        cost_estimate=cost(4 * heads * length * DK * DV, 4 * keys.size + 2 * values.size),
        name="cell_state",
    )(*deps, keys, values, in_gate, forget_gate)


def intra_kernel(queries, keys, values, rows, inner, stats, *, block, heads):
    length = queries.shape[0]
    rise = rows[0:SUB, :]
    peak = running_max(rise)
    peak_col = jnp.transpose(peak)
    scale = DK ** (-0.5)
    causal = lax.broadcasted_iota(jnp.int32, (block, block), 1) <= lax.broadcasted_iota(
        jnp.int32, (block, block), 0
    )
    place = lax.broadcasted_iota(jnp.int32, (block, SUB), 1)
    totals = []
    for first in range(0, length, block):
        seen = first + block
        kept = jnp.zeros((block, SUB), F32)
        for h in range(heads):
            r = h * SUB // heads
            ks, vs = slice(h * DK, (h + 1) * DK), slice(h * DV, (h + 1) * DV)
            q = (queries[first:seen, ks].astype(F32) * scale).astype(BF16)
            mu = peak_col[first:seen, r : r + 1]
            level = jnp.where(causal, rise[r : r + 1, first:seen] - mu, NEG)
            scores = dot_nt(q, keys[first:seen, ks]) * jnp.exp(level)
            total = jnp.sum(scores, axis=1, keepdims=True)
            part = dot(scores.astype(BF16), values[first:seen, vs])
            if first:
                scores = dot_nt(q, keys[0:first, ks]) * jnp.exp(rise[r : r + 1, 0:first] - mu)
                total = total + jnp.sum(scores, axis=1, keepdims=True)
                part = part + dot(scores.astype(BF16), values[0:first, vs])
            inner[first:seen, vs] = part
            kept = jnp.where(place * heads // SUB == h, total, kept)
        totals.append(kept)
    stats[0:SUB, :] = jnp.transpose(jnp.concatenate(totals, axis=0))
    stats[SUB : 2 * SUB, :] = peak


def cell_intra(queries, keys, values, rows, heads, deps=()):
    length = queries.shape[0]
    vm = pl.BlockSpec(memory_space=pltpu.VMEM)
    return pl.pallas_call(
        with_deps(functools.partial(intra_kernel, block=256, heads=heads), len(deps), 0),
        in_specs=anywhere(deps) + [vm] * 4,
        out_shape=[
            jax.ShapeDtypeStruct((length, heads * DV), F32),
            jax.ShapeDtypeStruct((2 * SUB, length), F32),
        ],
        compiler_params=params(),
        cost_estimate=cost(heads * length * length * (DK + DV), 8 * values.size, heads * length * length),
        name="cell_intra",
    )(*deps, queries, keys, values, rows)


def finish_kernel(ep_idx, *refs, n_packs, heads, block):
    packs, rest = refs[:n_packs], refs[n_packs:]
    queries, out_gate, gain, inner, stats, rows, mixed = rest
    me = ep_idx[0]
    base = heads * DK
    length = queries.shape[0]
    before = [jnp.bitwise_xor(me, k + 1) for k in range(n_packs)]
    decay = [p[base + 1 : base + 2, :] for p in packs]
    after = []
    anchor = jnp.zeros((1, LANES), F32)
    for k in range(n_packs):
        gone = jnp.zeros((1, LANES), F32)
        for other in range(n_packs):
            between = (before[other] > before[k]) & (before[other] < me)
            gone = gone + jnp.where(between, decay[other], 0.0)
        after.append(gone)
        anchor = anchor + jnp.where(before[k] < me, decay[k], 0.0)
    levels = [packs[k][base + 2 : base + 3, :] + after[k] for k in range(n_packs)]
    stab = anchor
    for k in range(n_packs):
        stab = jnp.maximum(stab, jnp.where(before[k] < me, levels[k], NEG))
    weights = [
        jnp.where(before[k] < me, jnp.exp(jnp.minimum(levels[k] - stab, 0.0)), 0.0)
        for k in range(n_packs)
    ]
    normal = jnp.zeros((1, LANES), F32)
    for k in range(n_packs):
        normal = normal + weights[k] * packs[k][base : base + 1, :]
    scale = DK ** (-0.5)
    total, peak, cum = stats[0:SUB, :], stats[SUB : 2 * SUB, :], rows[SUB : 2 * SUB, :]
    head_of = lax.broadcasted_iota(jnp.int32, (SUB, length), 0) * heads // SUB
    stab_in = jnp.broadcast_to(stab[:, 0:1], (SUB, length))
    normal_dot = jnp.zeros((SUB, length), F32)
    states = []
    for h in range(heads):
        ks = slice(h * DK, (h + 1) * DK)
        matrix = jnp.zeros((DK, DV), F32)
        for k in range(n_packs):
            matrix = matrix + weights[k][:, h * DK : h * DK + 1] * packs[k][ks, :]
        states.append(two_parts(matrix))
        n_high, n_low = two_parts(jnp.broadcast_to(normal[:, ks], (SUB, DK)))
        q = queries[:, ks]
        along = (dot_nt(n_high, q) + dot_nt(n_low, q)) * scale
        normal_dot = jnp.where(head_of == h, along, normal_dot)
        stab_in = jnp.where(head_of == h, stab[:, h * DK : h * DK + 1], stab_in)
    mu = jnp.maximum(peak, stab_in)
    here = jnp.exp(peak - mu)
    there = jnp.exp(stab_in - mu)
    divisor = jnp.maximum(jnp.abs(total * here + there * normal_dot), jnp.exp(-(cum + mu)))
    here_col = jnp.transpose(here / divisor)
    there_col = jnp.transpose(there / divisor * scale)
    for first in range(0, length, block):
        span = slice(first, first + block)
        for h in range(heads):
            r = h * SUB // heads
            cols, ks = slice(h * DV, (h + 1) * DV), slice(h * DK, (h + 1) * DK)
            q = queries[span, ks]
            across = dot(q, states[h][0]) + dot(q, states[h][1])
            cells = inner[span, cols] * here_col[span, r : r + 1] + across * there_col[span, r : r + 1]
            opened = jax.nn.sigmoid(out_gate[span, cols].astype(F32)) * gain[:, cols]
            mixed[span, cols] = (cells * opened).astype(BF16)


def cell_finish(ep_idx, packs, queries, out_gate, gain, inner, stats, rows, heads, deps=()):
    length, width = out_gate.shape
    vm = pl.BlockSpec(memory_space=pltpu.VMEM)
    return pl.pallas_call(
        with_deps(
            functools.partial(finish_kernel, n_packs=len(packs), heads=heads, block=256), len(deps), 1
        ),
        out_shape=jax.ShapeDtypeStruct((length, width), BF16),
        in_specs=[pl.BlockSpec(memory_space=pltpu.SMEM)]
        + anywhere(deps)
        + [vm] * (len(packs) + 6),
        compiler_params=params(),
        cost_estimate=cost(4 * heads * length * DK * DV, 12 * length * width, length * width),
        name="cell_finish",
    )(ep_idx, *deps, *packs, queries, out_gate, gain, inner, stats, rows)


def project_kernel(idx, *refs, n_tp, block):
    mixed, rest = refs[:n_tp], refs[n_tp:]
    share, low_part, high_part, out, joined, stage, sems = rest
    me = idx[0]
    _, part, _ = share.shape
    length = mixed[0].shape[0]
    half_tp = n_tp // 2
    for j in range(n_tp):
        source = me ^ j
        low = source < half_tp
        bit = jnp.where(low, idx[1], idx[2])
        first = j * 2 * part
        here = pl.ds(pl.multiple_of(first + bit * part, part), part)
        there = pl.ds(pl.multiple_of(first + (bit ^ 1) * part, part), part)
        joined[here, :] = share[source]

        @pl.when(low)
        def _():
            joined[there, :] = low_part[source]

        @pl.when(jnp.logical_not(low))
        def _():
            joined[there, :] = high_part[source - half_tp]

    leaving = []
    for b in range(length // block):
        rows = slice(b * block, (b + 1) * block)
        parts = [m[rows, :] for m in mixed]
        lhs = jnp.concatenate(parts, axis=1)
        stage[rows, :] = dot(lhs, joined[...]).astype(BF16)
        span = pl.ds(b * block, block)
        leaving += start_all(
            [pltpu.make_async_copy(stage.at[span, :], out.at[span, :], sems.at[b])]
        )
    wait_all(leaving)


def project(idx, mixed, share, low_part, high_part, deps=()):
    length, own = mixed[0].shape
    n_tp = share.shape[0]
    cols = share.shape[-1]
    block = 256
    hbm = pl.BlockSpec(memory_space=pl.ANY)
    vm = pl.BlockSpec(memory_space=pltpu.VMEM)
    return pl.pallas_call(
        with_deps(functools.partial(project_kernel, n_tp=n_tp, block=block), len(deps), 1),
        out_shape=jax.ShapeDtypeStruct((length, cols), BF16),
        in_specs=[pl.BlockSpec(memory_space=pltpu.SMEM)] + anywhere(deps) + [vm] * (len(mixed) + 3),
        out_specs=hbm,
        scratch_shapes=[
            pltpu.VMEM((n_tp * own, cols), BF16),
            pltpu.VMEM((length, cols), BF16),
            pltpu.SemaphoreType.DMA((length // block,)),
        ],
        compiler_params=params(20),
        cost_estimate=cost(2 * length * n_tp * own * cols, 2 * length * n_tp * own),
        name="project",
    )(idx, *deps, *mixed, share, low_part, high_part)


def passed_on(k, n_z):
    return n_z == 4 and k == 2


def local(
    queries,
    keys,
    values,
    out_gate,
    in_gate,
    forget_gate,
    out_gain,
    out_weight,
    moe_rows,
    moe_gain,
    routes,
    route_weight,
    expert_gate,
    expert_up,
    expert_down,
    shared_gate,
    shared_up,
    shared_down,
):
    n_tp, n_ep = lax.axis_size("tp"), lax.axis_size("ep")
    n_z = n_tp // 2
    me_tp, me_ep = lax.axis_index("tp"), lax.axis_index("ep")
    me_z, core = me_tp // 2, me_tp % 2
    heads = in_gate.shape[0]
    routed_rows, _ = moe_rows.shape
    topk = routes.shape[1]
    exact = 3 * routed_rows * topk // (2 * n_ep)
    cap = -(-exact // 16) * 16

    low_bit, high_bit = me_ep % 2, me_ep // (n_ep // 2)
    half_tp = n_tp // 2
    own_bit = jnp.where(me_tp < half_tp, low_bit, high_bit)
    idx = jnp.stack([me_ep, core, own_bit]).astype(jnp.int32)
    core_idx = core.reshape(1).astype(jnp.int32)
    z_idx = me_z.reshape(1).astype(jnp.int32)
    ep_idx = me_ep.reshape(1).astype(jnp.int32)

    normed, dest, share, outgoing = prep(
        idx,
        *put([moe_rows], pltpu.HBM),
        moe_gain.reshape(1, -1),
        routes.astype(jnp.int32).T,
        *put([out_weight], pltpu.HBM),
        n_ep,
        n_tp,
        cap,
    )
    arrived = [outgoing[0]]
    for k in range(1, n_ep):
        arrived.append(swap(outgoing[k], "ep", k))

    share = lax.all_to_all(share, "tp", 0, 0, tiled=True)

    pack, gate_info = cell_state(keys, values, in_gate, forget_gate, [dest])
    packs = []
    for k in range(1, n_ep):
        packs.append(swap(pack, "ep", k))
    inner, stats = cell_intra(queries, keys, values, gate_info, heads, [pack])
    mixed = cell_finish(
        ep_idx, put(packs, pltpu.VMEM), queries, out_gate, out_gain.reshape(1, -1), inner, stats, gate_info, heads
    )
    pieces, gathered = [], [mixed] + [None] * (n_z - 1)
    for k in range(1, n_z):
        if not passed_on(k, n_z):
            gathered[k] = swap(mixed, "tp", 2 * k)
    for k in range(1, n_z):
        if passed_on(k, n_z):
            gathered[k] = swap(gathered[n_z - 1], "tp", 2 * (n_z - 1 - k))
    for g in gathered:
        pieces += [g, swap(g, "tp", 1)]

    others = []
    for a in arrived:
        others.append(swap(a, "tp", 1))
    dest_cols = dest.T
    weight_cols = route_weight * jnp.ones((1, 1), F32)
    project_idx = jnp.stack([me_tp, low_bit, high_bit]).astype(jnp.int32)
    half_idx = jnp.stack([core, me_z // (n_z // 2)]).astype(jnp.int32)
    *sends, hidden = expert(
        half_idx, put(arrived, pltpu.VMEM), put(others, pltpu.VMEM), *put([expert_gate, expert_up, expert_down], pltpu.HBM), n_z, [mixed]
    )
    got = []
    for part in range(2):
        got.append(swap(sends[part], "tp", 1))
    backs, dep = [], hidden
    for part in range(2):
        sums = pair_sum(
            half_idx, hidden, *put([got[part]], pltpu.VMEM), *put([expert_down], pltpu.HBM), n_ep, n_z, part, [dep]
        )
        dep = sums[0]
        back = [sums[0]]
        for k in range(1, n_ep):
            back.append(swap(sums[k], "ep", k))
        backs.append(back)
    low_part = swap(share[:half_tp], "ep", 1)
    high_part = swap(share[half_tp:], "ep", n_ep // 2)
    shared_send, shared_own = shared(
        core_idx,
        normed,
        *put([shared_gate, shared_up, shared_down], pltpu.HBM),
        n_z,
        [dep, dest_cols, weight_cols, project_idx],
    )
    shared_other = swap(shared_send, "tp", 1)
    parts, total, dep = [None] * n_z, None, shared_own
    for part in range(2):
        outs = combine(
            z_idx, put(backs[part], pltpu.VMEM), shared_own, *put([shared_other], pltpu.VMEM), dest_cols, weight_cols, n_z, part, [dep]
        )
        dep = outs[0]
        first = 0 if part else n_z // 2
        parts[first : first + n_z // 2] = outs
    total = parts[0].astype(F32)
    for k in range(1, n_z):
        total = total + swap(parts[k], "tp", 2 * k).astype(F32)
    moe_out = total.astype(BF16)
    mixer_out = project(
        project_idx, put(pieces, pltpu.VMEM), *put([share, low_part, high_part], pltpu.VMEM), [dep]
    )
    return (mixer_out, moe_out)


def solution(mesh):
    return jax.shard_map(
        local,
        mesh=mesh,
        in_specs=(
            P("ep", "tp"),
            P("ep", "tp"),
            P("ep", "tp"),
            P("ep", "tp"),
            P("tp", "ep"),
            P("tp", "ep"),
            P("tp"),
            P("tp", None),
            P("ep", None),
            P(),
            P("ep", None),
            P("ep", None),
            P("ep", None, "tp"),
            P("ep", None, "tp"),
            P("ep", "tp", None),
            P(None, "tp"),
            P(None, "tp"),
            P("tp", None),
        ),
        out_specs=(P("ep", "tp"), P("ep", "tp")),
        check_vma=False,
    )
```
